32 devices in a mesh: grp: 2 (over x), ep: 8 (over z, y), tp: 2 (over core).
Axes of the slice: x: 2, y: 2, z: 4, core: 2. Of those that a mesh axis runs over, the one named last changes fastest.
Arguments:
- tokens: bfloat16 [8192, 2048], P(('grp', 'ep', 'tp')), parts along dimension 0, may hold values from -6 to 6
- norm_gain: float32 [2048], replicated, may hold values from 0.1 to 1.9
- route_ids: int32 [8192, 2], P(('grp', 'ep', 'tp')), parts along dimension 0, may hold values from 0 to 7, as said below
- route_weights: float32 [8192, 2], P(('grp', 'ep', 'tp')), parts along dimension 0, may hold values from 0.1 to 1
- w_gate: bfloat16 [8, 2048, 512], P('ep', None, 'tp'), may hold values from -0.125 to 0.125
- w_up: bfloat16 [8, 2048, 512], P('ep', None, 'tp'), may hold values from -0.125 to 0.125
- w_down: bfloat16 [8, 512, 2048], P('ep', 'tp'), may hold values from -0.25 to 0.25
Outputs:
- mixed: bfloat16 [8192, 2048], P(('grp', 'ep', 'tp')), parts along dimension 0
The draws below stay inside these ranges and needn't reach their ends.
There are 2 independent parts, one for each index of `grp`. The reference program is written for one: setup_inputs(seed, part) draws one part's arguments, and reference() takes and returns one part's arrays. A program takes and returns all parts, laid end to end along the dimension named above; an argument that names none is the same for every part. Nothing has to cross between parts.
Inputs may be any that keep to these rules, and one draw needn't show every extreme that they name: `route_ids`: the 2 experts of a token are different and lie in one group of 2 consecutive experts. Among the tokens of one device (aligned blocks of 256 tokens) no expert is named more than 128 times, and in every such block some expert is named exactly 128 times.
All inputs are finite; a program needn't handle non-finite values.
Results may differ from the reference program's by a relative error of at most 0.007.
Values may be sent and summed in bfloat16 or wider, within the bound.
A program may use at most 128 MiB of HBM per device.

```python
import math
import jax
import jax.numpy as jnp
from jax import lax

D = 2048
FF = 512
GROUPS = 4
TOPK = 2
TOK_DEV = 256
EXPERTS = 8
EXP_GROUP = 2
CAP = 128
TOKENS = 4096


def route_block(block_key):
    subkeys = jax.random.split(block_key, 5)
    halfway = TOK_DEV // 2
    busiest = jax.random.randint(subkeys[0], (), 0, GROUPS)
    spare = halfway - (GROUPS - 1) * EXP_GROUP
    cut_points = jnp.sort(jax.random.randint(subkeys[1], (GROUPS - 2,), 0, spare + 1))
    bounds = jnp.concatenate([jnp.zeros((1,), jnp.int32), cut_points.astype(jnp.int32), jnp.full((1,), spare, jnp.int32)])
    group_sizes = jnp.concatenate([jnp.full((1,), halfway, jnp.int32), bounds[1:] - bounds[:-1] + EXP_GROUP])
    bound_ends = jnp.cumsum(group_sizes)
    starts = bound_ends - group_sizes
    position = jnp.arange(TOK_DEV, dtype=jnp.int32)
    group_rank = jnp.sum((position[:, None] >= bound_ends[None, :]).astype(jnp.int32), axis=1)
    within = position - starts[group_rank]
    group = (busiest + group_rank) % GROUPS
    offsets = jax.random.randint(subkeys[2], (GROUPS,), 0, EXP_GROUP)
    shifts = jax.random.randint(subkeys[3], (GROUPS,), 1, EXP_GROUP)
    first_pick = (within + offsets[group]) % EXP_GROUP
    second_pick = (first_pick + shifts[group]) % EXP_GROUP
    chosen = group[:, None] * EXP_GROUP + jnp.stack([first_pick, second_pick], axis=1)
    shuffle = jax.random.permutation(subkeys[4], TOK_DEV)
    return jnp.zeros((TOK_DEV, 2), jnp.int32).at[shuffle].set(chosen.astype(jnp.int32))


def draw_route_ids(key, part):
    block_keys = jax.random.split(jax.random.fold_in(key, 17), TOKENS // TOK_DEV)
    return jax.vmap(route_block)(block_keys).reshape(TOKENS, TOPK).astype(jnp.int32)


def levels(rng, dims, pieces, smallest, high):
    gain, own = 1.0, jax.random.fold_in(rng, 6)
    for dim, shards_of in pieces:
        steps = jnp.exp(jax.random.uniform(jax.random.fold_in(own, dim), (shards_of,), jnp.float32, smallest / len(pieces), high / len(pieces)))
        gain = gain * jnp.repeat(steps, dims[dim] // shards_of).reshape([-1 if axis == dim else 1 for axis in range(len(dims))])
    return gain


def gaussian(rng, dims, width, reach, pieces=(), held_as=jnp.bfloat16):
    loudness = levels(rng, dims, pieces, -0.22, 0.18) if pieces else 1.0
    result = jax.random.normal(rng, dims, jnp.float32) * width * loudness
    return jnp.minimum(jnp.maximum(result, -reach), reach).astype(held_as)


def setup_inputs(seed: int = 0, part: int = 0) -> dict:
    streams_of = jax.random.split(jax.random.key(seed), 8)
    own_keys = jax.random.split(jax.random.fold_in(streams_of[7], part), 8)
    return {
        "tokens": gaussian(own_keys[0], (TOKENS, D), 1.0, 6.0, ((0, 16),)),
        "norm_gain": jnp.clip(1.0 + 0.18 * jax.random.normal(streams_of[1], (D,), jnp.float32), 0.1, 1.9),
        "route_ids": draw_route_ids(jax.random.fold_in(jax.random.fold_in(streams_of[7], part), 71), part),
        "route_weights": jnp.clip(jnp.exp(math.log(1.0) - 2.3025851 * jax.random.uniform(own_keys[3], (TOKENS, TOPK), jnp.float32) ** levels(own_keys[3], (TOKENS, TOPK), ((0, 16),), -0.2, 0.2)), 0.1, 1.0),
        "w_gate": gaussian(streams_of[4], (EXPERTS, D, FF), D ** -0.5, 0.125, ((0, 8), (2, 2))),
        "w_up": gaussian(streams_of[5], (EXPERTS, D, FF), D ** -0.5, 0.125, ((0, 8), (2, 2))),
        "w_down": gaussian(streams_of[6], (EXPERTS, FF, D), FF ** -0.5, 0.25, ((0, 8), (1, 2))),
    }


epsilon = 1e-06

def reference(tokens, norm_gain, route_ids, route_weights, w_gate, w_up, w_down):
    floats = tokens.astype(jnp.float32)
    inverse = lax.rsqrt(lax.optimization_barrier(jnp.mean(floats * floats, axis=1, keepdims=True)) + epsilon)
    normed = (floats * inverse * norm_gain.astype(jnp.float32)).astype(jnp.bfloat16)
    blocks = TOKENS // TOK_DEV
    route_flat = route_ids.reshape(blocks, TOK_DEV * TOPK).astype(jnp.int32)
    onehot = (route_flat[:, :, None] == jnp.arange(EXPERTS, dtype=jnp.int32)[None, None, :]).astype(jnp.int32)
    slot_index = lax.optimization_barrier(jnp.sum((jnp.cumsum(onehot, axis=1) - onehot) * onehot, axis=2)).astype(jnp.int32)
    anchor = jnp.arange(blocks, dtype=jnp.int32)[:, None]
    position = ((route_flat * blocks + anchor) * CAP + slot_index).astype(jnp.int32)
    position = position.reshape(TOKENS, TOPK)
    buffer = jnp.zeros((EXPERTS * blocks * CAP, D), jnp.bfloat16)
    for column in range(TOPK):
        buffer = buffer.at[position[:, column]].set(normed)
    buffer = buffer.reshape(EXPERTS, blocks * CAP, D)

    def expert(inputs):
        batch_rows, gate_weight, up_weight, down_weight = inputs
        gate_pre = jnp.dot(batch_rows, gate_weight, preferred_element_type=jnp.float32)
        up_pre = jnp.dot(batch_rows, up_weight, preferred_element_type=jnp.float32)
        hidden = (jax.nn.silu(gate_pre) * up_pre).astype(jnp.bfloat16)
        return jnp.dot(hidden, down_weight, preferred_element_type=jnp.float32).astype(jnp.bfloat16)
    results = lax.map(expert, (buffer, w_gate, w_up, w_down)).reshape(EXPERTS * blocks * CAP, D)
    combined = jnp.zeros((TOKENS, D), jnp.float32)
    for column in range(TOPK):
        picked = results[position[:, column]].astype(jnp.float32)
        combined = combined + route_weights[:, column:column + 1].astype(jnp.float32) * picked
    return combined.astype(jnp.bfloat16)
```

```python
import functools

import jax
import jax.numpy as jnp
from jax import lax
from jax.experimental import pallas as pl
from jax.experimental.pallas import tpu as pltpu
from jax.sharding import PartitionSpec as P

GROUPS = 4
EARLY = 1
SPLIT = 4
MESH = pl.DeviceIdType.MESH


epsilon = 1e-06


def send_back(result):
    return lax.all_to_all(result, "ep", split_axis=0, concat_axis=0, tiled=True)


def general_layer(tokens, norm_gain, route_ids, route_weights, w_gate, w_up, w_down):
    row_count, features = tokens.shape
    top_count = route_ids.shape[1]
    local_experts = w_gate.shape[0]
    ep_size = lax.axis_size("ep")
    experts_all = ep_size * local_experts
    capacity = row_count * GROUPS // experts_all
    floats = tokens.astype(jnp.float32)
    inverse = lax.rsqrt(jnp.mean(floats * floats, axis=1, keepdims=True) + epsilon)
    normed = (floats * inverse * norm_gain).astype(jnp.bfloat16)
    flat_ids = route_ids.reshape(-1)
    onehot = (flat_ids[:, None] == jnp.arange(experts_all, dtype=jnp.int32)[None, :]).astype(
        jnp.int32
    )
    earlier = jnp.cumsum(onehot, axis=0) - onehot
    slot_index = jnp.sum(earlier * onehot, axis=1)
    target = (flat_ids * capacity + slot_index).reshape(row_count, top_count)
    outbound = jnp.zeros((experts_all * capacity, features), jnp.bfloat16)
    for column in range(top_count):
        outbound = outbound.at[target[:, column]].set(normed)
    outbound = outbound.reshape(ep_size, local_experts, capacity, features)
    full_gate, full_up, full_down = (
        lax.all_gather(w_gate, "tp", axis=2, tiled=True),
        lax.all_gather(w_up, "tp", axis=2, tiled=True),
        lax.all_gather(w_down, "tp", axis=1, tiled=True),
    )
    arrived = lax.all_to_all(outbound, "ep", split_axis=0, concat_axis=0, tiled=True)
    gate_pre = jnp.einsum("sjcd,jdf->sjcf", arrived, full_gate, preferred_element_type=jnp.float32)
    up_pre = jnp.einsum("sjcd,jdf->sjcf", arrived, full_up, preferred_element_type=jnp.float32)
    hidden = (jax.nn.silu(gate_pre) * up_pre).astype(jnp.bfloat16)
    result = jnp.einsum("sjcf,jfd->sjcd", hidden, full_down, preferred_element_type=jnp.float32)
    returned_rows = send_back(result.astype(jnp.bfloat16))
    returned_rows = returned_rows.reshape(experts_all * capacity, features)
    combined = jnp.zeros((row_count, features), jnp.float32)
    for column in range(top_count):
        picked = returned_rows[target[:, column]].astype(jnp.float32)
        combined = combined + route_weights[:, column : column + 1] * picked
    return combined.astype(jnp.bfloat16)


def group_kernel(
    members, parts, halves,
    tokens, gain_in, ids_in, weights_in, w_gate, w_up, w_down, out,
    gain, ids, weights, raw, ready, summed, place, sent, taken, scales, scales_in, answers, returned,
    gate_all, up_all, down_all, hidden,
    raw_sem, small_sems, own_sems, twin_s, twin_r, peer_s, peer_r, part_s, part_r,
    near_s, near_r, far_s, far_r, row_s, row_r, scale_s, scale_r, back_s, back_r,
):
    part, position, half = lax.axis_index("grp"), lax.axis_index("ep"), lax.axis_index("tp")
    level, member = position // members, position % members
    rows, features = tokens.shape
    slots = sent.shape[1]
    top_count = ids.shape[0]
    peer = {"ep": level * members + (members - 1 - member)}
    other_part = {"grp": parts - 1 - part}
    twin = {"tp": halves - 1 - half}

    def level_of(k):
        return {"ep": (level ^ k) * members + member}

    barrier = pltpu.get_barrier_semaphore()
    neighbours = [level_of(k) for k in range(GROUPS - 1, 0, -1)] + [peer, other_part, twin]
    for device in neighbours:
        pl.semaphore_signal(barrier, inc=1, device_id=device, device_id_type=MESH)
    small_copies = [
        pltpu.make_async_copy(src, dst, small_sems.at[i])
        for i, (src, dst) in enumerate(((ids_in, ids), (weights_in, weights), (gain_in, gain)))
    ]
    raw_copy = pltpu.make_async_copy(tokens, raw, raw_sem)
    for copy in small_copies + [raw_copy]:
        copy.start()

    sources = (w_gate, w_up, w_down)
    stores = (gate_all, up_all, down_all)
    mine = member * halves + half
    theirs = (members - 1 - member) * halves + half

    def remote(src, dst, send, recv, device):
        return pltpu.make_async_remote_copy(
            src_ref=src, dst_ref=dst, send_sem=send, recv_sem=recv,
            device_id=device, device_id_type=MESH,
        )

    pieces = []
    for step in range(SPLIT):
        for tensor in range(3):
            size = sources[tensor].shape[0] // (parts * SPLIT)
            pieces.append((tensor, step, size))

    def span(index, which):
        tensor, step, size = pieces[index]
        start = pl.multiple_of((which * SPLIT + step) * size, size)
        return tensor, pl.ds(start, size)

    def peer_copy(index):
        tensor, window = span(index, part)
        return remote(
            sources[tensor].at[window], stores[tensor].at[mine, window],
            peer_s.at[index], peer_r.at[index], peer,
        )

    def spread_copy(index, which, send, recv, device):
        tensor, window = span(index, which)
        block = stores[tensor].at[theirs, window]
        return remote(block, block, send.at[index], recv.at[index], device)

    peer_copies = [peer_copy(index) for index in range(len(pieces))]
    part_copies = [spread_copy(i, part, part_s, part_r, other_part) for i in range(len(pieces))]
    near_copies = [spread_copy(i, part, near_s, near_r, twin) for i in range(len(pieces))]
    far_copies = [
        spread_copy(i, parts - 1 - part, far_s, far_r, twin) for i in range(len(pieces))
    ]
    own_copies, twin_copies = [], []
    for tensor in range(3):
        own_copies.append(
            pltpu.make_async_copy(sources[tensor], stores[tensor].at[mine], own_sems.at[tensor])
        )
        twin_copies.append(
            remote(
                sources[tensor], stores[tensor].at[mine],
                twin_s.at[tensor], twin_r.at[tensor], twin,
            )
        )
    for copy in small_copies:
        copy.wait()
    first = ids[0:1, :]
    group_row = first // members
    lane = lax.broadcasted_iota(jnp.int32, (8, rows), 0)
    mask = (jnp.broadcast_to(group_row, (8, rows)) == lane).astype(jnp.float32)
    before = (
        lax.broadcasted_iota(jnp.int32, (rows, rows), 0)
        < lax.broadcasted_iota(jnp.int32, (rows, rows), 1)
    ).astype(jnp.float32)
    ranks = jnp.dot(
        mask.astype(jnp.bfloat16), before.astype(jnp.bfloat16),
        preferred_element_type=jnp.float32,
    )
    slot_row = jnp.sum(ranks * mask, axis=0, keepdims=True).astype(jnp.int32)
    shares = jnp.zeros((8, rows), jnp.float32)
    for column in range(top_count):
        offset = ids[column : column + 1, :] - group_row * members
        chosen = jnp.broadcast_to(offset, (8, rows)) == lane
        shares = shares + jnp.where(
            chosen, jnp.broadcast_to(weights[column : column + 1, :], (8, rows)), 0.0
        )
    high = shares.astype(jnp.bfloat16)
    rest = shares - high.astype(jnp.float32)
    middle = rest.astype(jnp.bfloat16)
    low = (rest - middle.astype(jnp.float32)).astype(jnp.bfloat16)

    row_copies, scale_copies, back_copies = {}, {}, {}
    slot_iota = lax.broadcasted_iota(jnp.int32, (slots, rows), 0)
    order = (2, 1, 3, 0)
    for k in (1, 2, 3):
        row_copies[k] = remote(sent.at[k], taken.at[k], row_s.at[k], row_r.at[k], level_of(k))
        scale_copies[k] = remote(
            scales.at[k], scales_in.at[k], scale_s.at[k], scale_r.at[k], level_of(k)
        )

    def pack(k):
        key = jnp.where(group_row == (level ^ k), slot_row, -1)
        spots = (jnp.broadcast_to(key, (slots, rows)) == slot_iota).astype(jnp.float32)
        spots = spots.astype(jnp.bfloat16)
        place[k * slots : (k + 1) * slots, :] = spots
        lanes = sum(
            lax.dot_general(
                piece, spots, (((1,), (1,)), ((), ())), preferred_element_type=jnp.float32
            )
            for piece in (high, middle, low)
        )
        packed = taken if k == 0 else sent
        (scales_in if k == 0 else scales)[k] = lanes
        packed[k] = jnp.dot(spots, raw[...], preferred_element_type=jnp.float32).astype(
            jnp.bfloat16
        )

    raw_copy.wait()
    for k in order[:EARLY]:
        pack(k)
    pl.semaphore_wait(barrier, len(neighbours))
    for k in order:
        if k not in order[:EARLY]:
            pack(k)
        if k:
            row_copies[k].start()
            scale_copies[k].start()
        if k == order[0]:
            for copy in peer_copies + own_copies + twin_copies:
                copy.start()

    for index in range(len(pieces)):
        peer_copies[index].wait_recv()
        part_copies[index].start()
        near_copies[index].start()
        if index:
            part_copies[index - 1].wait_recv()
            far_copies[index - 1].start()
    part_copies[-1].wait_recv()
    far_copies[-1].start()

    width = gate_all.shape[2]
    diagonal = lax.broadcasted_iota(jnp.int32, (slots, slots), 0) == lax.broadcasted_iota(
        jnp.int32, (slots, slots), 1
    )
    tile = features // GROUPS

    strip = 32

    def norm(k):
        def norm_strip(index, carry):
            window = pl.ds(pl.multiple_of(index * strip, strip), strip)
            floats = taken[k, window, :].astype(jnp.float32)
            inverse = lax.rsqrt(jnp.mean(floats * floats, axis=1, keepdims=True) + epsilon)
            ready[window, :] = (floats * inverse * gain[...]).astype(jnp.bfloat16)
            return carry

        lax.fori_loop(0, slots // strip, norm_strip, 0)

    def widen(k, owner):
        lanes = scales_in[k, pl.ds(owner, 1), :]
        scale = jnp.sum(
            jnp.where(diagonal, jnp.broadcast_to(lanes, (slots, slots)), 0.0),
            axis=1, keepdims=True,
        )
        for side in range(halves):
            block = owner * halves + side
            gate = jnp.dot(ready[...], gate_all[block], preferred_element_type=jnp.float32)
            up = jnp.dot(ready[...], up_all[block], preferred_element_type=jnp.float32)
            hidden[:, pl.ds(pl.multiple_of(block * width, width), width)] = (
                gate / (1.0 + jnp.exp(-gate)) * up * scale
            ).astype(jnp.bfloat16)

    def narrow(k):
        for column in range(features // tile):
            window = slice(column * tile, (column + 1) * tile)
            total = jnp.zeros((slots, tile), jnp.float32)
            for block in range(members * halves):
                total += jnp.dot(
                    hidden[:, block * width : (block + 1) * width],
                    down_all[block, :, window],
                    preferred_element_type=jnp.float32,
                )
            if k:
                answers[k, :, window] = total.astype(jnp.bfloat16)
            else:
                returned[0, :, window] = total.astype(jnp.bfloat16)

    for copy in own_copies:
        copy.wait()
    for copy in twin_copies:
        copy.wait_recv()
    for k in order:
        if k:
            row_copies[k].wait_recv()
            scale_copies[k].wait_recv()
        norm(k)
        widen(k, member)
        if k == order[0]:
            for copy in near_copies + far_copies:
                copy.wait_recv()
        widen(k, members - 1 - member)
        narrow(k)
        if k:
            back_copies[k] = remote(
                answers.at[k], returned.at[k], back_s.at[k], back_r.at[k], level_of(k)
            )
            back_copies[k].start()

    def unpack(k, window):
        return lax.dot_general(
            place[k * slots : (k + 1) * slots, :], returned[k, :, window],
            (((0,), (0,)), ((), ())), preferred_element_type=jnp.float32,
        )

    tiles = [slice(start, start + tile) for start in range(0, features, tile)]
    for window in tiles:
        summed[:, window] = unpack(0, window)
    for k in order[:-1]:
        back_copies[k].wait_recv()
        for window in tiles:
            total = summed[:, window] + unpack(k, window)
            if k == order[-2]:
                out[:, window] = total.astype(jnp.bfloat16)
            else:
                summed[:, window] = total

    for copy in peer_copies + part_copies + near_copies + far_copies + twin_copies:
        copy.wait_send()
    for k in (1, 2, 3):
        row_copies[k].wait_send()
        scale_copies[k].wait_send()
        back_copies[k].wait_send()


def group_layer(members, tokens, norm_gain, route_ids, route_weights, w_gate, w_up, w_down):
    rows, features = tokens.shape
    parts, halves = lax.axis_size("grp"), lax.axis_size("tp")
    width = w_gate.shape[2]
    slots = rows // route_ids.shape[1]
    copies = 3 * SPLIT
    blocks = members * halves
    bf16, f32, dma = jnp.bfloat16, jnp.float32, pltpu.SemaphoreType.DMA
    vmem = pl.BlockSpec(memory_space=pltpu.VMEM)
    return pl.pallas_call(
        functools.partial(group_kernel, members, parts, halves),
        out_shape=pltpu.VMEM((rows, features), bf16),
        in_specs=[pl.BlockSpec(memory_space=pltpu.HBM)] * 7,
        out_specs=vmem,
        scratch_shapes=[
            pltpu.VMEM((1, features), f32),
            pltpu.VMEM(route_ids.shape[::-1], jnp.int32),
            pltpu.VMEM(route_ids.shape[::-1], f32),
            pltpu.VMEM((rows, features), bf16),
            pltpu.VMEM((slots, features), bf16),
            pltpu.VMEM((rows, features), f32),
            pltpu.VMEM((GROUPS * slots, rows), bf16),
            pltpu.VMEM((GROUPS, slots, features), bf16),
            pltpu.VMEM((GROUPS, slots, features), bf16),
            pltpu.VMEM((GROUPS, 8, slots), f32),
            pltpu.VMEM((GROUPS, 8, slots), f32),
            pltpu.VMEM((GROUPS, slots, features), bf16),
            pltpu.VMEM((GROUPS, slots, features), bf16),
            pltpu.VMEM((blocks, features, width), bf16),
            pltpu.VMEM((blocks, features, width), bf16),
            pltpu.VMEM((blocks, width, features), bf16),
            pltpu.VMEM((slots, blocks * width), bf16),
            dma, dma((3,)), dma((3,)), dma((3,)), dma((3,)),
        ]
        + [dma((copies,)) for _ in range(8)]
        + [dma((GROUPS,)) for _ in range(6)],
        compiler_params=pltpu.CompilerParams(
            collective_id=0, has_side_effects=True, vmem_limit_bytes=64400 * 1024
        ),
    )(
        tokens, norm_gain.reshape(1, features), route_ids.T, route_weights.T,
        w_gate[0], w_up[0], w_down[0],
    )


def solution(mesh):
    sizes = mesh.shape

    def per_device(tokens, norm_gain, route_ids, route_weights, w_gate, w_up, w_down):
        arguments = (tokens, norm_gain, route_ids, route_weights, w_gate, w_up, w_down)
        members = sizes["ep"] * w_gate.shape[0] // GROUPS
        paired = members == route_ids.shape[1] == sizes["grp"] == sizes["tp"] == 2
        if paired and w_gate.shape[0] == 1:
            return group_layer(members, *arguments)
        return general_layer(*arguments)

    in_specs = (
        P(("grp", "ep", "tp"), None),
        P(),
        P(("grp", "ep", "tp"), None),
        P(("grp", "ep", "tp"), None),
        P("ep", None, "tp"),
        P("ep", None, "tp"),
        P("ep", "tp", None),
    )
    out_specs = P(("grp", "ep", "tp"), None)
    return jax.shard_map(
        per_device, mesh=mesh, in_specs=in_specs, out_specs=out_specs, check_vma=False
    )
```

```python
import functools

import jax
import jax.numpy as jnp
from jax import lax
from jax.experimental import pallas as pl
from jax.experimental.pallas import tpu as pltpu
from jax.sharding import PartitionSpec as P

GROUPS = 4
SPLIT = 4
SWAP_AT = 11
MESH = pl.DeviceIdType.MESH


epsilon = 1e-06


def send_back(result):
    return lax.all_to_all(result, "ep", split_axis=0, concat_axis=0, tiled=True)


def general_layer(tokens, norm_gain, route_ids, route_weights, w_gate, w_up, w_down):
    row_count, features = tokens.shape
    top_count = route_ids.shape[1]
    local_experts = w_gate.shape[0]
    ep_size = lax.axis_size("ep")
    experts_all = ep_size * local_experts
    capacity = row_count * GROUPS // experts_all
    floats = tokens.astype(jnp.float32)
    inverse = lax.rsqrt(jnp.mean(floats * floats, axis=1, keepdims=True) + epsilon)
    normed = (floats * inverse * norm_gain).astype(jnp.bfloat16)
    flat_ids = route_ids.reshape(-1)
    onehot = (flat_ids[:, None] == jnp.arange(experts_all, dtype=jnp.int32)[None, :]).astype(
        jnp.int32
    )
    earlier = jnp.cumsum(onehot, axis=0) - onehot
    slot_index = jnp.sum(earlier * onehot, axis=1)
    target = (flat_ids * capacity + slot_index).reshape(row_count, top_count)
    outbound = jnp.zeros((experts_all * capacity, features), jnp.bfloat16)
    for column in range(top_count):
        outbound = outbound.at[target[:, column]].set(normed)
    outbound = outbound.reshape(ep_size, local_experts, capacity, features)
    full_gate, full_up, full_down = (
        lax.all_gather(w_gate, "tp", axis=2, tiled=True),
        lax.all_gather(w_up, "tp", axis=2, tiled=True),
        lax.all_gather(w_down, "tp", axis=1, tiled=True),
    )
    arrived = lax.all_to_all(outbound, "ep", split_axis=0, concat_axis=0, tiled=True)
    gate_pre = jnp.einsum("sjcd,jdf->sjcf", arrived, full_gate, preferred_element_type=jnp.float32)
    up_pre = jnp.einsum("sjcd,jdf->sjcf", arrived, full_up, preferred_element_type=jnp.float32)
    hidden = (jax.nn.silu(gate_pre) * up_pre).astype(jnp.bfloat16)
    result = jnp.einsum("sjcf,jfd->sjcd", hidden, full_down, preferred_element_type=jnp.float32)
    returned_rows = send_back(result.astype(jnp.bfloat16))
    returned_rows = returned_rows.reshape(experts_all * capacity, features)
    combined = jnp.zeros((row_count, features), jnp.float32)
    for column in range(top_count):
        picked = returned_rows[target[:, column]].astype(jnp.float32)
        combined = combined + route_weights[:, column : column + 1] * picked
    return combined.astype(jnp.bfloat16)


def group_kernel(
    members, parts, halves,
    tokens, gain_in, ids_in, weights_in, w_gate, w_up, w_down, out,
    gain, ids, weights, raw, ready, summed, place, sent, taken, scales, scales_in, answers,
    returned, gate_all, up_all, down_all, hidden,
    own_gate, own_up, own_down, peer_rows, peer_scales, partial, parts_out, parts_in,
    raw_sem, small_sems, own_sems, twin_s, twin_r, peer_s, peer_r, part_s, part_r,
    near_s, near_r, far_s, far_r, guest_s, guest_r, cross_s, cross_r,
    gnear_s, gnear_r, gfar_s, gfar_r, row_s, row_r, scale_s, scale_r, back_s, back_r,
    swap_s, swap_r, note_s, note_r, half_s, half_r,
):
    part, position, half = lax.axis_index("grp"), lax.axis_index("ep"), lax.axis_index("tp")
    level, member = position // members, position % members
    inner = ((level + 1) // 2) % 2
    rows, features = tokens.shape
    slots = sent.shape[1]
    top_count = ids.shape[0]
    peer = {"ep": level * members + (members - 1 - member)}
    other_part = {"grp": parts - 1 - part}
    twin = {"tp": halves - 1 - half}

    def level_of(k):
        return {"ep": (level ^ k) * members + member}

    on_inner, on_outer = pl.when(inner == 1), pl.when(inner == 0)

    barrier = pltpu.get_barrier_semaphore()
    neighbours = [level_of(k) for k in range(GROUPS - 1, 0, -1)] + [peer, other_part, twin]
    for device in neighbours:
        pl.semaphore_signal(barrier, inc=1, device_id=device, device_id_type=MESH)
    small_copies = [
        pltpu.make_async_copy(src, dst, small_sems.at[i])
        for i, (src, dst) in enumerate(((ids_in, ids), (weights_in, weights), (gain_in, gain)))
    ]
    raw_copy = pltpu.make_async_copy(tokens, raw, raw_sem)
    for copy in small_copies + [raw_copy]:
        copy.start()

    sources = (w_gate, w_up, w_down)
    stores = (gate_all, up_all, down_all)
    own_stores = (own_gate, own_up, own_down)
    mine = member * halves + half
    theirs = (members - 1 - member) * halves + half

    def remote(src, dst, send, recv, device):
        return pltpu.make_async_remote_copy(
            src_ref=src, dst_ref=dst, send_sem=send, recv_sem=recv,
            device_id=device, device_id_type=MESH,
        )

    pieces = [(tensor, step) for step in range(SPLIT) for tensor in range(2)]
    pieces += [(2, step) for step in range(SPLIT)]
    count = len(pieces)
    wide = 2 * SPLIT

    def window_of(piece, which):
        tensor, step = piece
        size = sources[tensor].shape[0] // (parts * SPLIT)
        return pl.ds(pl.multiple_of((which * SPLIT + step) * size, size), size)

    def first_copies(send, recv, device):
        copies = []
        for i, piece in enumerate(pieces):
            window = window_of(piece, part)
            copies.append(remote(
                sources[piece[0]].at[window], stores[piece[0]].at[mine, window],
                send.at[i], recv.at[i], device,
            ))
        return copies

    def spread_copies(block, which, send, recv, device):
        copies = []
        for i, piece in enumerate(pieces):
            held = stores[piece[0]].at[block, window_of(piece, which)]
            copies.append(remote(held, held, send.at[i], recv.at[i], device))
        return copies

    other = parts - 1 - part
    peer_copies = first_copies(peer_s, peer_r, peer)
    relay_copies = spread_copies(mine, part, peer_s, peer_r, peer)
    part_copies = spread_copies(theirs, part, part_s, part_r, other_part)
    near_copies = spread_copies(theirs, part, near_s, near_r, twin)
    far_copies = spread_copies(theirs, other, far_s, far_r, twin)
    guest_copies = first_copies(guest_s, guest_r, level_of(GROUPS - 1))
    cross_copies = spread_copies(mine, part, cross_s, cross_r, other_part)
    gnear_copies = spread_copies(mine, part, gnear_s, gnear_r, twin)
    gfar_copies = spread_copies(mine, other, gfar_s, gfar_r, twin)

    def home_copies(targets, block):
        copies, twins = [], []
        for tensor in range(3):
            target = targets[tensor].at[block]
            copies.append(
                pltpu.make_async_copy(sources[tensor], target, own_sems.at[tensor])
            )
            twins.append(
                remote(sources[tensor], target, twin_s.at[tensor], twin_r.at[tensor], twin)
            )
        return copies, twins

    group_copies, group_twins = home_copies(stores, mine)
    own_copies, own_twins = home_copies(own_stores, half)
    row_to = {1: level_of(1), 2: level_of(1 + inner), 3: level_of(3)}
    back_to = {1: level_of(1), 2: level_of(2 - inner), 3: level_of(3)}
    tile = features // GROUPS
    tiles = [slice(begin, begin + tile) for begin in range(0, features, tile)]

    def tiled_copies(src, dst, send, recv, base, device):
        return [
            remote(
                src.at[:, window], dst.at[:, window],
                send.at[base * GROUPS + t], recv.at[base * GROUPS + t], device,
            )
            for t, window in enumerate(tiles)
        ]

    row_copies, scale_copies, back_copies = {}, {}, {}
    for k in (1, 2, 3):
        row_copies[k] = tiled_copies(sent.at[k], taken.at[k], row_s, row_r, k, row_to[k])
        scale_copies[k] = remote(
            scales.at[k], scales_in.at[k], scale_s.at[k], scale_r.at[k], row_to[k]
        )
        back_copies[k] = tiled_copies(answers.at[k], returned.at[k], back_s, back_r, k, back_to[k])
    swap_copies, note_copies, half_copies = [], [], []
    for j, k in enumerate((1, 0)):
        swap_copies.append(tiled_copies(taken.at[k], peer_rows.at[j], swap_s, swap_r, j, peer))
        note_copies.append(
            remote(scales_in.at[k], peer_scales.at[j], note_s.at[j], note_r.at[j], peer)
        )
        half_copies.append(tiled_copies(parts_out.at[j], parts_in.at[j], half_s, half_r, j, peer))

    for copy in small_copies:
        copy.wait()
    first = ids[0:1, :]
    group_row = first // members
    lane = lax.broadcasted_iota(jnp.int32, (8, rows), 0)
    mask = (jnp.broadcast_to(group_row, (8, rows)) == lane).astype(jnp.float32)
    before = (
        lax.broadcasted_iota(jnp.int32, (rows, rows), 0)
        < lax.broadcasted_iota(jnp.int32, (rows, rows), 1)
    ).astype(jnp.float32)
    ranks = jnp.dot(
        mask.astype(jnp.bfloat16), before.astype(jnp.bfloat16),
        preferred_element_type=jnp.float32,
    )
    slot_row = jnp.sum(ranks * mask, axis=0, keepdims=True).astype(jnp.int32)
    shares = jnp.zeros((8, rows), jnp.float32)
    for column in range(top_count):
        offset = ids[column : column + 1, :] - group_row * members
        chosen = jnp.broadcast_to(offset, (8, rows)) == lane
        shares = shares + jnp.where(
            chosen, jnp.broadcast_to(weights[column : column + 1, :], (8, rows)), 0.0
        )
    high = shares.astype(jnp.bfloat16)
    rest = shares - high.astype(jnp.float32)
    middle = rest.astype(jnp.bfloat16)
    low = (rest - middle.astype(jnp.float32)).astype(jnp.bfloat16)
    slot_iota = lax.broadcasted_iota(jnp.int32, (slots, rows), 0)

    def pack(k):
        key = jnp.where(group_row == (level ^ k), slot_row, -1)
        spots = (jnp.broadcast_to(key, (slots, rows)) == slot_iota).astype(jnp.float32)
        spots = spots.astype(jnp.bfloat16)
        place[k * slots : (k + 1) * slots, :] = spots
        lanes = sum(
            lax.dot_general(
                piece, spots, (((1,), (1,)), ((), ())), preferred_element_type=jnp.float32
            )
            for piece in (high, middle, low)
        )
        packed = taken if k == 0 else sent
        (scales_in if k == 0 else scales)[k] = lanes
        packed[k] = jnp.dot(spots, raw[...], preferred_element_type=jnp.float32).astype(
            jnp.bfloat16
        )

    def start(copies):
        for copy in copies:
            copy.start()

    def land(copies):
        for copy in copies:
            copy.wait_recv()

    def leave(copies):
        for copy in copies:
            copy.wait_send()

    def send(k):
        scale_copies[k].start()
        start(row_copies[k])

    def arrive(k):
        land(row_copies[k] + [scale_copies[k]])

    raw_copy.wait()
    pack(1)
    pl.semaphore_wait(barrier, len(neighbours))

    @on_inner
    def _():
        start(guest_copies)

    send(1)

    @on_outer
    def _():
        start(peer_copies)

    pack(0)

    @on_inner
    def _():
        start(own_copies + own_twins)

    @on_outer
    def _():
        start(group_copies + group_twins)

    pack(2)
    send(2)
    pack(3)

    width = gate_all.shape[2]
    diagonal = lax.broadcasted_iota(jnp.int32, (slots, slots), 0) == lax.broadcasted_iota(
        jnp.int32, (slots, slots), 1
    )
    strip = 32

    def norm(source, base):
        def norm_strip(index, carry):
            start = pl.multiple_of(index * strip, strip)
            floats = source[pl.ds(start, strip), :].astype(jnp.float32)
            inverse = lax.rsqrt(jnp.mean(floats * floats, axis=1, keepdims=True) + epsilon)
            ready[pl.ds(base + start, strip), :] = (floats * inverse * gain[...]).astype(
                jnp.bfloat16
            )
            return carry

        lax.fori_loop(0, slots // strip, norm_strip, 0)

    def column_of(share, owner):
        return jnp.sum(
            jnp.where(diagonal, jnp.broadcast_to(share[pl.ds(owner, 1), :], (slots, slots)), 0.0),
            axis=1, keepdims=True,
        )

    def widen(base, shares_in, owner, gate_block, up_block, column):
        scale = jnp.concatenate([column_of(share, owner) for share in shares_in], axis=0)
        size = slots * len(shares_in)
        values = ready[base : base + size, :]
        gate = jnp.dot(values, gate_block[...], preferred_element_type=jnp.float32)
        up = jnp.dot(values, up_block[...], preferred_element_type=jnp.float32)
        hidden[base : base + size, pl.ds(pl.multiple_of(column * width, width), width)] = (
            gate / (1.0 + jnp.exp(-gate)) * up * scale
        ).astype(jnp.bfloat16)

    def widen_group(base, shares_in, owner, side):
        block = owner * halves + side
        widen(base, shares_in, owner, gate_all.at[block], up_all.at[block], block)

    def narrow(base, size, blocks, column):
        window = slice(column * tile, (column + 1) * tile)
        total = jnp.zeros((size, tile), jnp.float32)
        for index, block in enumerate(blocks):
            total += jnp.dot(
                hidden[base : base + size, index * width : (index + 1) * width],
                block[:, window], preferred_element_type=jnp.float32,
            )
        return window, total

    group_down = [down_all.at[block] for block in range(members * halves)]

    def narrow_group(base, targets):
        for column in range(len(tiles)):
            window, total = narrow(base, slots * len(targets), group_down, column)
            for j, (target, copies) in enumerate(targets):
                target[:, window] = total[j * slots : (j + 1) * slots].astype(jnp.bfloat16)
                if copies:
                    copies[column].start()

    def whole(pair, base):
        for j, k in enumerate(pair):
            norm(taken.at[k], base + j * slots)
        for owner in range(members):
            for side in range(halves):
                widen_group(base, [scales_in.at[k] for k in pair], owner, side)
        narrow_group(
            base, [((answers if k else returned).at[k], back_copies.get(k)) for k in pair]
        )

    def divided(j, k):
        base = 2 * slots * j
        norm(peer_rows.at[j], base)
        norm(taken.at[k], base + slots)
        for side in range(halves):
            widen(
                base, [peer_scales.at[j], scales_in.at[k]], member,
                own_gate.at[side], own_up.at[side], side,
            )
        blocks = [own_down.at[side] for side in range(halves)]
        for column in range(len(tiles)):
            window, total = narrow(base, 2 * slots, blocks, column)
            parts_out[j, :, window] = total[:slots].astype(jnp.bfloat16)
            half_copies[j][column].start()
            partial[j, :, window] = total[slots:]

    def joined(j, column, target, copies=None):
        half_copies[j][column].wait_recv()
        window = tiles[column]
        target[:, window] = (
            partial[j, :, window] + parts_in[j, :, window].astype(jnp.float32)
        ).astype(jnp.bfloat16)
        if copies:
            copies[column].start()

    def unpack(k, window):
        return lax.dot_general(
            place[k * slots : (k + 1) * slots, :], returned[k, :, window],
            (((0,), (0,)), ((), ())), preferred_element_type=jnp.float32,
        )

    def add(k, fresh=False):
        for window in tiles:
            value = unpack(k, window)
            summed[:, window] = value if fresh else summed[:, window] + value

    def back(k):
        for t, window in enumerate(tiles):
            back_copies[k][t].wait_recv()
            summed[:, window] = summed[:, window] + unpack(k, window)

    def finish(k):
        for t, window in enumerate(tiles):
            back_copies[k][t].wait_recv()
            out[:, window] = (summed[:, window] + unpack(k, window)).astype(jnp.bfloat16)

    @on_outer
    def _():
        for i in range(count):
            peer_copies[i].wait_recv()
            part_copies[i].start()
            near_copies[i].start()
            if i:
                part_copies[i - 1].wait_recv()
                far_copies[i - 1].start()
        part_copies[-1].wait_recv()
        far_copies[-1].start()
        for copy in group_copies:
            copy.wait()
        land(group_twins + near_copies + far_copies)
        arrive(1)
        whole((1, 0), 2 * slots)
        send(3)
        add(0, True)
        arrive(2)
        whole((2,), 0)
        arrive(3)
        whole((3,), slots)
        back(1)
        back(3)
        finish(2)
        leave(peer_copies + group_twins + row_copies[3] + [scale_copies[3]] + back_copies[3])

    @on_inner
    def _():
        def take(i):
            guest_copies[i].wait_recv()
            cross_copies[i].start()
            gnear_copies[i].start()

        scale_copies[1].wait_recv()
        note_copies[0].start()
        for i in range(GROUPS):
            row_copies[1][i].wait_recv()
            swap_copies[0][i].start()
            take(i)
        relay_copies[0].start()
        take(GROUPS)
        for copy in own_copies:
            copy.wait()
        land(own_twins + swap_copies[0] + note_copies[:1])
        divided(0, 1)
        start(relay_copies[1 : GROUPS + 1])
        for i in range(GROUPS + 1, count):
            take(i)
            relay_copies[i].start()
            column = i - GROUPS - 1
            if column < GROUPS:
                joined(0, column, answers.at[1], back_copies[1])
            if i == SWAP_AT:
                note_copies[1].start()
                start(swap_copies[1])
        arrive(2)
        shares_in = [scales_in.at[2], scales.at[3]]
        norm(taken.at[2], 0)
        norm(sent.at[3], slots)
        for i in range(count):
            peer_copies[i].wait_recv()
            part_copies[i].start()
            near_copies[i].start()
            cross_copies[i].wait_recv()
            gfar_copies[i].start()
            if i:
                part_copies[i - 1].wait_recv()
                far_copies[i - 1].start()
            if i == wide:
                land(gnear_copies[:wide] + gfar_copies[:wide])
            if i == wide + members:
                land(near_copies[:wide] + far_copies[:wide])
            if i >= wide:
                owner, side = (i - wide) // halves, (i - wide) % halves
                widen_group(0, shares_in, (member + owner) % members, side)
        part_copies[-1].wait_recv()
        far_copies[-1].start()
        land(
            gnear_copies[wide:] + gfar_copies[wide:] + near_copies[wide:] + far_copies[wide:]
        )
        narrow_group(0, [(answers.at[2], back_copies[2]), (returned.at[3], None)])
        land(swap_copies[1] + note_copies[1:])
        divided(1, 0)
        add(3, True)
        back(1)
        back(2)
        for column, window in enumerate(tiles):
            joined(1, column, returned.at[0])
            out[:, window] = (summed[:, window] + unpack(0, window)).astype(jnp.bfloat16)
        leave(guest_copies + cross_copies + gnear_copies + gfar_copies + relay_copies)
        leave(own_twins + note_copies)
        for j in range(2):
            leave(swap_copies[j] + half_copies[j])

    leave(part_copies + near_copies + far_copies)
    for k in (1, 2):
        leave(row_copies[k] + [scale_copies[k]] + back_copies[k])


def group_layer(members, tokens, norm_gain, route_ids, route_weights, w_gate, w_up, w_down):
    rows, features = tokens.shape
    parts, halves = lax.axis_size("grp"), lax.axis_size("tp")
    width = w_gate.shape[2]
    slots = rows // route_ids.shape[1]
    copies = 3 * SPLIT
    blocks = members * halves
    bf16, f32, dma = jnp.bfloat16, jnp.float32, pltpu.SemaphoreType.DMA

    def vmem(*shape, dtype=bf16):
        return pltpu.VMEM(shape, dtype)

    return pl.pallas_call(
        functools.partial(group_kernel, members, parts, halves),
        out_shape=vmem(rows, features),
        in_specs=[pl.BlockSpec(memory_space=pltpu.HBM)] * 7,
        out_specs=pl.BlockSpec(memory_space=pltpu.VMEM),
        scratch_shapes=[
            vmem(1, features, dtype=f32),
            vmem(*route_ids.shape[::-1], dtype=jnp.int32),
            vmem(*route_ids.shape[::-1], dtype=f32),
            vmem(rows, features),
            vmem(GROUPS * slots, features),
            vmem(rows, features, dtype=f32),
            vmem(GROUPS * slots, rows),
            vmem(GROUPS, slots, features),
            vmem(GROUPS, slots, features),
            vmem(GROUPS, 8, slots, dtype=f32),
            vmem(GROUPS, 8, slots, dtype=f32),
            vmem(GROUPS, slots, features),
            vmem(GROUPS, slots, features),
            vmem(blocks, features, width),
            vmem(blocks, features, width),
            vmem(blocks, width, features),
            vmem(GROUPS * slots, blocks * width),
            vmem(halves, features, width),
            vmem(halves, features, width),
            vmem(halves, width, features),
            vmem(2, slots, features),
            vmem(2, 8, slots, dtype=f32),
            vmem(2, slots, features, dtype=f32),
            vmem(2, slots, features),
            vmem(2, slots, features),
            dma, dma((3,)), dma((3,)), dma((3,)), dma((3,)),
        ]
        + [dma((copies,)) for _ in range(16)]
        + [dma((GROUPS * GROUPS,)) for _ in range(2)]
        + [dma((GROUPS,)) for _ in range(2)]
        + [dma((GROUPS * GROUPS,)) for _ in range(2)]
        + [dma((2 * GROUPS,)) for _ in range(2)]
        + [dma((2,)) for _ in range(2)]
        + [dma((2 * GROUPS,)) for _ in range(2)],
        compiler_params=pltpu.CompilerParams(
            collective_id=0, has_side_effects=True, vmem_limit_bytes=64400 * 1024
        ),
    )(
        tokens, norm_gain.reshape(1, features), route_ids.T, route_weights.T,
        w_gate[0], w_up[0], w_down[0],
    )


def solution(mesh):
    sizes = mesh.shape

    def per_device(tokens, norm_gain, route_ids, route_weights, w_gate, w_up, w_down):
        arguments = (tokens, norm_gain, route_ids, route_weights, w_gate, w_up, w_down)
        members = sizes["ep"] * w_gate.shape[0] // GROUPS
        paired = members == route_ids.shape[1] == sizes["grp"] == sizes["tp"] == 2
        if paired and w_gate.shape[0] == 1:
            return group_layer(members, *arguments)
        return general_layer(*arguments)

    in_specs = (
        P(("grp", "ep", "tp"), None),
        P(),
        P(("grp", "ep", "tp"), None),
        P(("grp", "ep", "tp"), None),
        P("ep", None, "tp"),
        P("ep", None, "tp"),
        P("ep", "tp", None),
    )
    out_specs = P(("grp", "ep", "tp"), None)
    return jax.shard_map(
        per_device, mesh=mesh, in_specs=in_specs, out_specs=out_specs, check_vma=False
    )
```

```python
import functools

import jax
import jax.numpy as jnp
from jax import lax
from jax.experimental import pallas as pl
from jax.experimental.pallas import tpu as pltpu
from jax.sharding import PartitionSpec as P

GROUPS = 4
SPLIT = 4
MESH = pl.DeviceIdType.MESH


epsilon = 1e-06


def send_back(result):
    return lax.all_to_all(result, "ep", split_axis=0, concat_axis=0, tiled=True)


def general_layer(tokens, norm_gain, route_ids, route_weights, w_gate, w_up, w_down):
    row_count, features = tokens.shape
    top_count = route_ids.shape[1]
    local_experts = w_gate.shape[0]
    ep_size = lax.axis_size("ep")
    experts_all = ep_size * local_experts
    capacity = row_count * GROUPS // experts_all
    floats = tokens.astype(jnp.float32)
    inverse = lax.rsqrt(jnp.mean(floats * floats, axis=1, keepdims=True) + epsilon)
    normed = (floats * inverse * norm_gain).astype(jnp.bfloat16)
    flat_ids = route_ids.reshape(-1)
    onehot = (flat_ids[:, None] == jnp.arange(experts_all, dtype=jnp.int32)[None, :]).astype(
        jnp.int32
    )
    earlier = jnp.cumsum(onehot, axis=0) - onehot
    slot_index = jnp.sum(earlier * onehot, axis=1)
    target = (flat_ids * capacity + slot_index).reshape(row_count, top_count)
    outbound = jnp.zeros((experts_all * capacity, features), jnp.bfloat16)
    for column in range(top_count):
        outbound = outbound.at[target[:, column]].set(normed)
    outbound = outbound.reshape(ep_size, local_experts, capacity, features)
    full_gate, full_up, full_down = (
        lax.all_gather(w_gate, "tp", axis=2, tiled=True),
        lax.all_gather(w_up, "tp", axis=2, tiled=True),
        lax.all_gather(w_down, "tp", axis=1, tiled=True),
    )
    arrived = lax.all_to_all(outbound, "ep", split_axis=0, concat_axis=0, tiled=True)
    gate_pre = jnp.einsum("sjcd,jdf->sjcf", arrived, full_gate, preferred_element_type=jnp.float32)
    up_pre = jnp.einsum("sjcd,jdf->sjcf", arrived, full_up, preferred_element_type=jnp.float32)
    hidden = (jax.nn.silu(gate_pre) * up_pre).astype(jnp.bfloat16)
    result = jnp.einsum("sjcf,jfd->sjcd", hidden, full_down, preferred_element_type=jnp.float32)
    returned_rows = send_back(result.astype(jnp.bfloat16))
    returned_rows = returned_rows.reshape(experts_all * capacity, features)
    combined = jnp.zeros((row_count, features), jnp.float32)
    for column in range(top_count):
        picked = returned_rows[target[:, column]].astype(jnp.float32)
        combined = combined + route_weights[:, column : column + 1] * picked
    return combined.astype(jnp.bfloat16)


def group_kernel(
    members, parts, halves,
    tokens, gain_in, ids_in, weights_in, w_gate, w_up, w_down, out,
    gain, ids, weights, raw, ready, summed, place, sent, taken, scales, scales_in, answers, returned,
    gate_all, up_all, down_all, hidden,
    raw_sem, small_sems, peer_s, peer_r, part_s, part_r, twin_s, twin_r,
    row_s, row_r, scale_s, scale_r, back_s, back_r,
):
    part, position, half = lax.axis_index("grp"), lax.axis_index("ep"), lax.axis_index("tp")
    level, member = position // members, position % members
    rows, features = tokens.shape
    slots = sent.shape[1]
    top_count = ids.shape[0]
    peer = {"ep": level * members + (members - 1 - member)}
    other_part = {"grp": parts - 1 - part}
    twin = {"tp": halves - 1 - half}

    def level_of(k):
        return {"ep": (level ^ k) * members + member}

    barrier = pltpu.get_barrier_semaphore()
    neighbours = [level_of(k) for k in range(GROUPS - 1, 0, -1)] + [peer, other_part, twin]
    for device in neighbours:
        pl.semaphore_signal(barrier, inc=1, device_id=device, device_id_type=MESH)
    small_copies = [
        pltpu.make_async_copy(src, dst, small_sems.at[i])
        for i, (src, dst) in enumerate(((ids_in, ids), (weights_in, weights), (gain_in, gain)))
    ]
    raw_copy = pltpu.make_async_copy(tokens, raw, raw_sem)
    for copy in small_copies + [raw_copy]:
        copy.start()

    sources = (w_gate, w_up, w_down)
    stores = (gate_all, up_all, down_all)
    mine = member * halves + half
    theirs = (members - 1 - member) * halves + half

    def remote(src, dst, send, recv, device):
        return pltpu.make_async_remote_copy(
            src_ref=src, dst_ref=dst, send_sem=send, recv_sem=recv,
            device_id=device, device_id_type=MESH,
        )

    pieces = []
    for step in range(SPLIT):
        for tensor in range(3):
            size = sources[tensor].shape[0] // (parts * SPLIT)
            pieces.append((tensor, step, size))

    def span(index, which):
        tensor, step, size = pieces[index]
        start = pl.multiple_of((which * SPLIT + step) * size, size)
        return tensor, pl.ds(start, size)

    def peer_copy(index):
        tensor, window = span(index, part)
        return remote(
            sources[tensor].at[window], stores[tensor].at[mine, window],
            peer_s.at[tensor], peer_r.at[index], peer,
        )

    def spread_copy(index, which, send, recv, device):
        tensor, window = span(index, which)
        block = stores[tensor].at[theirs, window]
        return remote(block, block, send.at[tensor], recv, device)

    indices = range(len(pieces))
    peer_copies = [peer_copy(index) for index in indices]
    part_copies = [spread_copy(i, part, part_s, part_r.at[i], other_part) for i in indices]
    near_copies = [spread_copy(i, part, twin_s, twin_r.at[i % 3], twin) for i in indices]
    far_copies = [spread_copy(i, parts - 1 - part, twin_s, twin_r.at[i % 3], twin) for i in indices]
    own_copies, twin_copies, twin_all, half_all = [], [], [], []
    for tensor in range(3):
        own = stores[tensor].at[mine]
        own_copies.append(pltpu.make_async_copy(sources[tensor], own, small_sems.at[tensor]))
        twin_copies.append(
            remote(sources[tensor], own, twin_s.at[tensor], twin_r.at[tensor], twin)
        )
        both = stores[tensor].at[0:2]
        twin_all.append(remote(both, both, twin_s.at[tensor], twin_r.at[tensor], twin))
        piece = stores[tensor].at[0, 0 : sources[tensor].shape[0] // parts]
        for send, device in ((peer_s, peer), (part_s, other_part)):
            half_all.append(remote(piece, piece, send.at[tensor], peer_r.at[0], device))
    for copy in small_copies:
        copy.wait()
    first = ids[0:1, :]
    group_row = first // members
    lane = lax.broadcasted_iota(jnp.int32, (8, rows), 0)
    mask = (jnp.broadcast_to(group_row, (8, rows)) == lane).astype(jnp.float32)
    before = (
        lax.broadcasted_iota(jnp.int32, (rows, rows), 0)
        < lax.broadcasted_iota(jnp.int32, (rows, rows), 1)
    ).astype(jnp.float32)
    ranks = jnp.dot(
        mask.astype(jnp.bfloat16), before.astype(jnp.bfloat16),
        preferred_element_type=jnp.float32,
    )
    slot_row = jnp.sum(ranks * mask, axis=0, keepdims=True).astype(jnp.int32)
    shares = jnp.zeros((8, rows), jnp.float32)
    for column in range(top_count):
        offset = ids[column : column + 1, :] - group_row * members
        chosen = jnp.broadcast_to(offset, (8, rows)) == lane
        shares = shares + jnp.where(
            chosen, jnp.broadcast_to(weights[column : column + 1, :], (8, rows)), 0.0
        )
    high = shares.astype(jnp.bfloat16)
    rest = shares - high.astype(jnp.float32)
    middle = rest.astype(jnp.bfloat16)
    low = (rest - middle.astype(jnp.float32)).astype(jnp.bfloat16)

    tile = features // GROUPS
    order = (2, 1, 3, 0)
    tiles = [slice(begin, begin + tile) for begin in range(0, features, tile)]
    row_copies, scale_copies, back_copies = {}, {}, {}
    slot_iota = lax.broadcasted_iota(jnp.int32, (slots, rows), 0)
    for k in (1, 2, 3):
        row_copies[k] = remote(
            sent.at[k], taken.at[k], row_s, row_r.at[k - 1], level_of(k)
        )
        scale_copies[k] = remote(
            scales.at[k, :members], scales_in.at[k, :members],
            scale_s, scale_r.at[k - 1], level_of(k),
        )

        cut = tiles if k == order[-2] else [slice(0, features)]
        back_copies[k] = [
            remote(
                answers.at[k, :, window], returned.at[k, :, window],
                back_s, back_r.at[k - 1 + t], level_of(k),
            )
            for t, window in enumerate(cut)
        ]

    def pack(k):
        key = jnp.where(group_row == (level ^ k), slot_row, -1)
        spots = (jnp.broadcast_to(key, (slots, rows)) == slot_iota).astype(jnp.float32)
        spots = spots.astype(jnp.bfloat16)
        place[k * slots : (k + 1) * slots, :] = spots
        lanes = sum(
            lax.dot_general(
                piece, spots, (((1,), (1,)), ((), ())), preferred_element_type=jnp.float32
            )
            for piece in (high, middle, low)
        )
        packed = taken if k == 0 else sent
        (scales_in if k == 0 else scales)[k] = lanes
        packed[k] = jnp.dot(spots, raw[...], preferred_element_type=jnp.float32).astype(
            jnp.bfloat16
        )

    raw_copy.wait()
    pack(order[0])
    pl.semaphore_wait(barrier, len(neighbours))
    for k in order:
        if k != order[0]:
            pack(k)
        if k:
            scale_copies[k].start()
            row_copies[k].start()
        if k == order[0]:
            for copy in peer_copies + own_copies + twin_copies:
                copy.start()

    for index in range(len(pieces)):
        peer_copies[index].wait_recv()
        part_copies[index].start()
        near_copies[index].start()
        if index:
            part_copies[index - 1].wait_recv()
            far_copies[index - 1].start()
    part_copies[-1].wait_recv()
    far_copies[-1].start()

    width = gate_all.shape[2]
    diagonal = lax.broadcasted_iota(jnp.int32, (slots, slots), 0) == lax.broadcasted_iota(
        jnp.int32, (slots, slots), 1
    )

    strip = 32

    def norm(k):
        def norm_strip(index, carry):
            window = pl.ds(pl.multiple_of(index * strip, strip), strip)
            floats = taken[k, window, :].astype(jnp.float32)
            inverse = lax.rsqrt(jnp.mean(floats * floats, axis=1, keepdims=True) + epsilon)
            ready[window, :] = (floats * inverse * gain[...]).astype(jnp.bfloat16)
            return carry

        lax.fori_loop(0, slots // strip, norm_strip, 0)

    def widen(k, owner):
        lanes = scales_in[k, pl.ds(owner, 1), :]
        scale = jnp.sum(
            jnp.where(diagonal, jnp.broadcast_to(lanes, (slots, slots)), 0.0),
            axis=1, keepdims=True,
        )
        for side in range(halves):
            block = owner * halves + side
            gate = jnp.dot(ready[...], gate_all[block], preferred_element_type=jnp.float32)
            up = jnp.dot(ready[...], up_all[block], preferred_element_type=jnp.float32)
            hidden[:, pl.ds(pl.multiple_of(block * width, width), width)] = (
                gate / (1.0 + jnp.exp(-gate)) * up * scale
            ).astype(jnp.bfloat16)

    def narrow(k):
        for column, window in enumerate(tiles):
            total = jnp.zeros((slots, tile), jnp.float32)
            for block in range(members * halves):
                total += jnp.dot(
                    hidden[:, block * width : (block + 1) * width],
                    down_all[block, :, window],
                    preferred_element_type=jnp.float32,
                )
            if k:
                answers[k, :, window] = total.astype(jnp.bfloat16)
                if k == order[-2]:
                    back_copies[k][column].start()
            else:
                returned[0, :, window] = total.astype(jnp.bfloat16)

    for copy in own_copies:
        copy.wait()
    for copy in twin_all:
        copy.wait_recv()
    for k in order:
        if k:
            row_copies[k].wait_recv()
            scale_copies[k].wait_recv()
        norm(k)
        widen(k, member)
        widen(k, members - 1 - member)
        narrow(k)
        if k and k != order[-2]:
            back_copies[k][0].start()

    def unpack(k, window):
        return lax.dot_general(
            place[k * slots : (k + 1) * slots, :], returned[k, :, window],
            (((0,), (0,)), ((), ())), preferred_element_type=jnp.float32,
        )

    for window in tiles:
        summed[:, window] = unpack(0, window)
    for k in order[:-1]:
        for t, window in enumerate(tiles):
            if t < len(back_copies[k]):
                back_copies[k][t].wait_recv()
            total = summed[:, window] + unpack(k, window)
            if k == order[-2]:
                out[:, window] = total.astype(jnp.bfloat16)
            else:
                summed[:, window] = total

    for copy in half_all + twin_all:
        copy.wait_send()
    for buffer, sem in ((sent, row_s), (scales, scale_s), (answers, back_s)):
        used = buffer.at[1:GROUPS] if sem is not scale_s else buffer.at[1:GROUPS, :members]
        remote(used, used, sem, back_r.at[0], twin).wait_send()


def group_layer(members, tokens, norm_gain, route_ids, route_weights, w_gate, w_up, w_down):
    rows, features = tokens.shape
    parts, halves = lax.axis_size("grp"), lax.axis_size("tp")
    width = w_gate.shape[2]
    slots = rows // route_ids.shape[1]
    copies = 3 * SPLIT
    blocks = members * halves
    bf16, f32, dma = jnp.bfloat16, jnp.float32, pltpu.SemaphoreType.DMA
    vmem = pl.BlockSpec(memory_space=pltpu.VMEM)
    return pl.pallas_call(
        functools.partial(group_kernel, members, parts, halves),
        out_shape=pltpu.VMEM((rows, features), bf16),
        in_specs=[pl.BlockSpec(memory_space=pltpu.HBM)] * 7,
        out_specs=vmem,
        scratch_shapes=[
            pltpu.VMEM((1, features), f32),
            pltpu.VMEM(route_ids.shape[::-1], jnp.int32),
            pltpu.VMEM(route_ids.shape[::-1], f32),
            pltpu.VMEM((rows, features), bf16),
            pltpu.VMEM((slots, features), bf16),
            pltpu.VMEM((rows, features), f32),
            pltpu.VMEM((GROUPS * slots, rows), bf16),
            pltpu.VMEM((GROUPS, slots, features), bf16),
            pltpu.VMEM((GROUPS, slots, features), bf16),
            pltpu.VMEM((GROUPS, 8, slots), f32),
            pltpu.VMEM((GROUPS, 8, slots), f32),
            pltpu.VMEM((GROUPS, slots, features), bf16),
            pltpu.VMEM((GROUPS, slots, features), bf16),
            pltpu.VMEM((blocks, features, width), bf16),
            pltpu.VMEM((blocks, features, width), bf16),
            pltpu.VMEM((blocks, width, features), bf16),
            pltpu.VMEM((slots, blocks * width), bf16),
            dma, dma((3,)), dma((3,)), dma((copies,)), dma((3,)), dma((copies,)),
            dma((3,)), dma((3,)), dma, dma((3,)), dma, dma((3,)), dma, dma((6,)),
        ],
        compiler_params=pltpu.CompilerParams(
            collective_id=0, has_side_effects=True, vmem_limit_bytes=64400 * 1024
        ),
    )(
        tokens, norm_gain.reshape(1, features), route_ids.T, route_weights.T,
        w_gate[0], w_up[0], w_down[0],
    )


def solution(mesh):
    sizes = mesh.shape

    def per_device(tokens, norm_gain, route_ids, route_weights, w_gate, w_up, w_down):
        arguments = (tokens, norm_gain, route_ids, route_weights, w_gate, w_up, w_down)
        members = sizes["ep"] * w_gate.shape[0] // GROUPS
        paired = members == route_ids.shape[1] == sizes["grp"] == sizes["tp"] == 2
        if paired and w_gate.shape[0] == 1:
            return group_layer(members, *arguments)
        return general_layer(*arguments)

    in_specs = (
        P(("grp", "ep", "tp"), None),
        P(),
        P(("grp", "ep", "tp"), None),
        P(("grp", "ep", "tp"), None),
        P("ep", None, "tp"),
        P("ep", None, "tp"),
        P("ep", "tp", None),
    )
    out_specs = P(("grp", "ep", "tp"), None)
    return jax.shard_map(
        per_device, mesh=mesh, in_specs=in_specs, out_specs=out_specs, check_vma=False
    )
```

```python
import functools

import jax
import jax.numpy as jnp
from jax import lax
from jax.experimental import pallas as pl
from jax.experimental.pallas import tpu as pltpu
from jax.sharding import PartitionSpec as P

GROUPS = 4
SPLIT = 4
MESH = pl.DeviceIdType.MESH


epsilon = 1e-06


def send_back(result):
    return lax.all_to_all(result, "ep", split_axis=0, concat_axis=0, tiled=True)


def general_layer(tokens, norm_gain, route_ids, route_weights, w_gate, w_up, w_down):
    row_count, features = tokens.shape
    top_count = route_ids.shape[1]
    local_experts = w_gate.shape[0]
    ep_size = lax.axis_size("ep")
    experts_all = ep_size * local_experts
    capacity = row_count * GROUPS // experts_all
    floats = tokens.astype(jnp.float32)
    inverse = lax.rsqrt(jnp.mean(floats * floats, axis=1, keepdims=True) + epsilon)
    normed = (floats * inverse * norm_gain).astype(jnp.bfloat16)
    flat_ids = route_ids.reshape(-1)
    onehot = (flat_ids[:, None] == jnp.arange(experts_all, dtype=jnp.int32)[None, :]).astype(
        jnp.int32
    )
    earlier = jnp.cumsum(onehot, axis=0) - onehot
    slot_index = jnp.sum(earlier * onehot, axis=1)
    target = (flat_ids * capacity + slot_index).reshape(row_count, top_count)
    outbound = jnp.zeros((experts_all * capacity, features), jnp.bfloat16)
    for column in range(top_count):
        outbound = outbound.at[target[:, column]].set(normed)
    outbound = outbound.reshape(ep_size, local_experts, capacity, features)
    full_gate, full_up, full_down = (
        lax.all_gather(w_gate, "tp", axis=2, tiled=True),
        lax.all_gather(w_up, "tp", axis=2, tiled=True),
        lax.all_gather(w_down, "tp", axis=1, tiled=True),
    )
    arrived = lax.all_to_all(outbound, "ep", split_axis=0, concat_axis=0, tiled=True)
    gate_pre = jnp.einsum("sjcd,jdf->sjcf", arrived, full_gate, preferred_element_type=jnp.float32)
    up_pre = jnp.einsum("sjcd,jdf->sjcf", arrived, full_up, preferred_element_type=jnp.float32)
    hidden = (jax.nn.silu(gate_pre) * up_pre).astype(jnp.bfloat16)
    result = jnp.einsum("sjcf,jfd->sjcd", hidden, full_down, preferred_element_type=jnp.float32)
    returned_rows = send_back(result.astype(jnp.bfloat16))
    returned_rows = returned_rows.reshape(experts_all * capacity, features)
    combined = jnp.zeros((row_count, features), jnp.float32)
    for column in range(top_count):
        picked = returned_rows[target[:, column]].astype(jnp.float32)
        combined = combined + route_weights[:, column : column + 1] * picked
    return combined.astype(jnp.bfloat16)


def group_kernel(
    members, parts, halves,
    tokens, gain_in, ids_in, weights_in, w_gate, w_up, w_down, out,
    gain, ids, weights, raw, ready, summed, place, sent, taken, scales, scales_in, answers,
    returned,
    gate_all, up_all, down_all, hidden,
    raw_sems, small_sems, peer_r, part_r, twin_r, weight_s, row_s, row_r, scale_s, scale_r,
    back_s, back_r,
):
    part, position, half = lax.axis_index("grp"), lax.axis_index("ep"), lax.axis_index("tp")
    level, member = position // members, position % members
    rows, features = tokens.shape
    slots = sent.shape[1]
    top_count = ids.shape[0]
    peer = {"ep": level * members + (members - 1 - member)}
    other_part = {"grp": parts - 1 - part}
    twin = {"tp": halves - 1 - half}

    def level_of(k):
        return {"ep": (level ^ k) * members + member}

    barrier = pltpu.get_barrier_semaphore()
    neighbours = [level_of(k) for k in range(GROUPS - 1, 0, -1)] + [peer, other_part, twin]
    for device in neighbours:
        pl.semaphore_signal(barrier, inc=1, device_id=device, device_id_type=MESH)
    tile = features // GROUPS
    tiles = [slice(begin, begin + tile) for begin in range(0, features, tile)]
    small_copies = [
        pltpu.make_async_copy(src, dst, small_sems.at[i])
        for i, (src, dst) in enumerate(((ids_in, ids), (weights_in, weights), (gain_in, gain)))
    ]
    raw_copies = []
    for i, window in enumerate((tiles[0], slice(tile, features))):
        raw_copies.append(
            pltpu.make_async_copy(tokens.at[:, window], raw.at[:, window], raw_sems.at[i])
        )
    for copy in small_copies[:1] + raw_copies + small_copies[1:]:
        copy.start()

    sources = (w_gate, w_up, w_down)
    stores = (gate_all, up_all, down_all)
    mine = member * halves + half
    theirs = (members - 1 - member) * halves + half

    def remote(src, dst, send, recv, device):
        return pltpu.make_async_remote_copy(
            src_ref=src, dst_ref=dst, send_sem=send, recv_sem=recv,
            device_id=device, device_id_type=MESH,
        )

    pieces = []
    for step in range(SPLIT):
        for tensor in range(3):
            size = sources[tensor].shape[0] // (parts * SPLIT)
            pieces.append((tensor, step, size))

    def span(index, which):
        tensor, step, size = pieces[index]
        start = pl.multiple_of((which * SPLIT + step) * size, size)
        return tensor, pl.ds(start, size)

    def peer_copy(index):
        tensor, window = span(index, part)
        return remote(
            sources[tensor].at[window], stores[tensor].at[mine, window],
            weight_s.at[tensor], peer_r.at[index], peer,
        )

    def spread_copy(index, which, recv, device):
        tensor, window = span(index, which)
        block = stores[tensor].at[theirs, window]
        return remote(block, block, weight_s.at[tensor], recv, device)

    indices = range(len(pieces))
    peer_copies = [peer_copy(index) for index in indices]
    part_copies = [spread_copy(i, part, part_r.at[i], other_part) for i in indices]
    near_copies = [spread_copy(i, part, twin_r.at[i % 3], twin) for i in indices]
    far_copies = [spread_copy(i, parts - 1 - part, twin_r.at[i % 3], twin) for i in indices]
    own_copies, twin_copies, twin_all, sent_all = [], [], [], []
    for tensor in range(3):
        own = stores[tensor].at[mine]
        own_copies.append(pltpu.make_async_copy(sources[tensor], own, small_sems.at[tensor]))
        twin_copies.append(
            remote(sources[tensor], own, weight_s.at[tensor], twin_r.at[tensor], twin)
        )
        for blocks, waits in ((2, twin_all), (3, sent_all)):
            span_all = stores[tensor].at[0:blocks]
            waits.append(
                remote(span_all, span_all, weight_s.at[tensor], twin_r.at[tensor], twin)
            )
    lane = lax.broadcasted_iota(jnp.int32, (8, rows), 0)
    before = (
        lax.broadcasted_iota(jnp.int32, (rows, rows), 0)
        < lax.broadcasted_iota(jnp.int32, (rows, rows), 1)
    ).astype(jnp.float32).astype(jnp.bfloat16)
    slot_iota = lax.broadcasted_iota(jnp.int32, (slots, rows), 0)
    small_copies[0].wait()
    first = ids[0:1, :]
    group_row = first // members
    mask = (jnp.broadcast_to(group_row, (8, rows)) == lane).astype(jnp.float32)
    ranks = jnp.dot(mask.astype(jnp.bfloat16), before, preferred_element_type=jnp.float32)
    slot_row = jnp.sum(ranks * mask, axis=0, keepdims=True).astype(jnp.int32)
    order = (2, 1, 3, 0)
    row_copies, scale_copies, back_copies = {}, {}, {}
    for k in (1, 2, 3):
        row_copies[k] = [
            remote(
                sent.at[k, :, window], taken.at[k, :, window],
                row_s, row_r.at[k - 1], level_of(k),
            )
            for window in (tiles if k == order[0] else [slice(0, features)])
        ]
        scale_copies[k] = remote(
            scales.at[k, :members], scales_in.at[k, :members],
            scale_s, scale_r, level_of(k),
        )

        cut = tiles if k == order[-2] else [slice(0, features)]
        back_copies[k] = [
            remote(
                answers.at[k, :, window], returned.at[k, :, window],
                back_s, back_r.at[k - 1 + t], level_of(k),
            )
            for t, window in enumerate(cut)
        ]

    def find(k):
        key = jnp.where(group_row == (level ^ k), slot_row, -1)
        spots = (jnp.broadcast_to(key, (slots, rows)) == slot_iota).astype(jnp.float32)
        spots = spots.astype(jnp.bfloat16)
        place[k * slots : (k + 1) * slots, :] = spots
        return spots

    def pack(k, spots, window):
        packed = taken if k == 0 else sent
        packed[k, :, window] = jnp.dot(
            spots, raw[:, window], preferred_element_type=jnp.float32
        ).astype(jnp.bfloat16)

    early = order[0]
    spots = find(early)
    raw_copies[0].wait()
    pack(early, spots, tiles[0])
    pl.semaphore_wait(barrier, len(neighbours))
    row_copies[early][0].start()
    for copy in peer_copies:
        copy.start()
    raw_copies[1].wait()
    for window, copy in zip(tiles[1:], row_copies[early][1:]):
        pack(early, spots, window)
        copy.start()
    for copy in small_copies[1:]:
        copy.wait()
    found = {k: find(k) for k in order[1:]}
    shares = jnp.zeros((8, rows), jnp.float32)
    for column in range(top_count):
        offset = ids[column : column + 1, :] - group_row * members
        chosen = jnp.broadcast_to(offset, (8, rows)) == lane
        shares = shares + jnp.where(
            chosen, jnp.broadcast_to(weights[column : column + 1, :], (8, rows)), 0.0
        )
    high = shares.astype(jnp.bfloat16)
    rest = shares - high.astype(jnp.float32)
    middle = rest.astype(jnp.bfloat16)
    low = (rest - middle.astype(jnp.float32)).astype(jnp.bfloat16)
    for k in order:
        (scales if k else scales_in)[k] = sum(
            lax.dot_general(
                piece, place[k * slots : (k + 1) * slots, :], (((1,), (1,)), ((), ())),
                preferred_element_type=jnp.float32,
            )
            for piece in (high, middle, low)
        )
        if k:
            scale_copies[k].start()

    for k in order[1:]:
        pack(k, found[k], slice(0, features))
        if k:
            row_copies[k][0].start()
    for copy in own_copies + twin_copies:
        copy.start()

    for index in range(len(pieces)):
        peer_copies[index].wait_recv()
        part_copies[index].start()
        near_copies[index].start()
        if index:
            part_copies[index - 1].wait_recv()
            far_copies[index - 1].start()
    part_copies[-1].wait_recv()
    far_copies[-1].start()

    width = gate_all.shape[2]
    diagonal = lax.broadcasted_iota(jnp.int32, (slots, slots), 0) == lax.broadcasted_iota(
        jnp.int32, (slots, slots), 1
    )

    strip = 32

    def norm(k):
        def norm_strip(index, carry):
            window = pl.ds(pl.multiple_of(index * strip, strip), strip)
            floats = taken[k, window, :].astype(jnp.float32)
            inverse = lax.rsqrt(jnp.mean(floats * floats, axis=1, keepdims=True) + epsilon)
            ready[window, :] = (floats * inverse * gain[...]).astype(jnp.bfloat16)
            return carry

        lax.fori_loop(0, slots // strip, norm_strip, 0)

    def widen(k, owner):
        lanes = scales_in[k, pl.ds(owner, 1), :]
        scale = jnp.sum(
            jnp.where(diagonal, jnp.broadcast_to(lanes, (slots, slots)), 0.0),
            axis=1, keepdims=True,
        )
        for side in range(halves):
            block = owner * halves + side
            gate = jnp.dot(ready[...], gate_all[block], preferred_element_type=jnp.float32)
            up = jnp.dot(ready[...], up_all[block], preferred_element_type=jnp.float32)
            hidden[:, pl.ds(pl.multiple_of(block * width, width), width)] = (
                gate / (1.0 + jnp.exp(-gate)) * up * scale
            ).astype(jnp.bfloat16)

    def narrow(k):
        for column, window in enumerate(tiles):
            total = jnp.zeros((slots, tile), jnp.float32)
            for block in range(members * halves):
                total += jnp.dot(
                    hidden[:, block * width : (block + 1) * width],
                    down_all[block, :, window],
                    preferred_element_type=jnp.float32,
                )
            if k:
                answers[k, :, window] = total.astype(jnp.bfloat16)
                if k == order[-2]:
                    back_copies[k][column].start()
            else:
                returned[0, :, window] = total.astype(jnp.bfloat16)

    for copy in own_copies:
        copy.wait()
    scale_all = scales.at[1:GROUPS, :members]
    scale_all = remote(scale_all, scale_all, scale_s, scale_r, twin)
    for copy in twin_all + [scale_all]:
        copy.wait_recv()
    for k in order:
        if k:
            remote(sent.at[k], taken.at[k], row_s, row_r.at[k - 1], twin).wait_recv()
        norm(k)
        widen(k, member)
        widen(k, members - 1 - member)
        narrow(k)
        if k and k != order[-2]:
            back_copies[k][0].start()

    def unpack(k, window):
        return lax.dot_general(
            place[k * slots : (k + 1) * slots, :], returned[k, :, window],
            (((0,), (0,)), ((), ())), preferred_element_type=jnp.float32,
        )

    for window in tiles:
        summed[:, window] = unpack(0, window)
    for k in order[:-1]:
        for t, window in enumerate(tiles):
            if t < len(back_copies[k]):
                back_copies[k][t].wait_recv()
            total = summed[:, window] + unpack(k, window)
            if k == order[-2]:
                out[:, window] = total.astype(jnp.bfloat16)
            else:
                summed[:, window] = total

    for buffer, sem in ((sent, row_s), (answers, back_s)):
        flows = buffer.at[1:GROUPS]
        sent_all.append(remote(flows, flows, sem, back_r.at[0], twin))
    for copy in sent_all + [scale_all]:
        copy.wait_send()


def group_layer(members, tokens, norm_gain, route_ids, route_weights, w_gate, w_up, w_down):
    rows, features = tokens.shape
    parts, halves = lax.axis_size("grp"), lax.axis_size("tp")
    width = w_gate.shape[2]
    slots = rows // route_ids.shape[1]
    copies = 3 * SPLIT
    blocks = members * halves
    bf16, f32, dma = jnp.bfloat16, jnp.float32, pltpu.SemaphoreType.DMA
    vmem = pl.BlockSpec(memory_space=pltpu.VMEM)
    return pl.pallas_call(
        functools.partial(group_kernel, members, parts, halves),
        out_shape=pltpu.VMEM((rows, features), bf16),
        in_specs=[pl.BlockSpec(memory_space=pltpu.HBM)] * 7,
        out_specs=vmem,
        scratch_shapes=[
            pltpu.VMEM((1, features), f32),
            pltpu.VMEM(route_ids.shape[::-1], jnp.int32),
            pltpu.VMEM(route_ids.shape[::-1], f32),
            pltpu.VMEM((rows, features), bf16),
            pltpu.VMEM((slots, features), bf16),
            pltpu.VMEM((rows, features), f32),
            pltpu.VMEM((GROUPS * slots, rows), bf16),
            pltpu.VMEM((GROUPS, slots, features), bf16),
            pltpu.VMEM((GROUPS, slots, features), bf16),
            pltpu.VMEM((GROUPS, 8, slots), f32),
            pltpu.VMEM((GROUPS, 8, slots), f32),
            pltpu.VMEM((GROUPS, slots, features), bf16),
            pltpu.VMEM((GROUPS, slots, features), bf16),
            pltpu.VMEM((blocks, features, width), bf16),
            pltpu.VMEM((blocks, features, width), bf16),
            pltpu.VMEM((blocks, width, features), bf16),
            pltpu.VMEM((slots, blocks * width), bf16),
            dma((2,)), dma((3,)), dma((copies,)), dma((copies,)), dma((3,)), dma((3,)),
            dma, dma((3,)), dma, dma, dma, dma((6,)),
        ],
        compiler_params=pltpu.CompilerParams(
            collective_id=0, has_side_effects=True, vmem_limit_bytes=64400 * 1024
        ),
    )(
        tokens, norm_gain.reshape(1, features), route_ids.T, route_weights.T,
        w_gate[0], w_up[0], w_down[0],
    )


def solution(mesh):
    sizes = mesh.shape

    def per_device(tokens, norm_gain, route_ids, route_weights, w_gate, w_up, w_down):
        arguments = (tokens, norm_gain, route_ids, route_weights, w_gate, w_up, w_down)
        members = sizes["ep"] * w_gate.shape[0] // GROUPS
        paired = members == route_ids.shape[1] == sizes["grp"] == sizes["tp"] == 2
        if paired and w_gate.shape[0] == 1:
            return group_layer(members, *arguments)
        return general_layer(*arguments)

    in_specs = (
        P(("grp", "ep", "tp"), None),
        P(),
        P(("grp", "ep", "tp"), None),
        P(("grp", "ep", "tp"), None),
        P("ep", None, "tp"),
        P("ep", None, "tp"),
        P("ep", "tp", None),
    )
    out_specs = P(("grp", "ep", "tp"), None)
    return jax.shard_map(
        per_device, mesh=mesh, in_specs=in_specs, out_specs=out_specs, check_vma=False
    )
```

```python
import functools

import jax
import jax.numpy as jnp
from jax import lax
from jax.experimental import pallas as pl
from jax.experimental.pallas import tpu as pltpu
from jax.sharding import PartitionSpec as P

GROUPS = 4
SPLIT = 4
HELD = 0
LATE = 7
FIRST = True
MESH = pl.DeviceIdType.MESH


epsilon = 1e-06


def send_back(result):
    return lax.all_to_all(result, "ep", split_axis=0, concat_axis=0, tiled=True)


def general_layer(tokens, norm_gain, route_ids, route_weights, w_gate, w_up, w_down):
    row_count, features = tokens.shape
    top_count = route_ids.shape[1]
    local_experts = w_gate.shape[0]
    ep_size = lax.axis_size("ep")
    experts_all = ep_size * local_experts
    capacity = row_count * GROUPS // experts_all
    floats = tokens.astype(jnp.float32)
    inverse = lax.rsqrt(jnp.mean(floats * floats, axis=1, keepdims=True) + epsilon)
    normed = (floats * inverse * norm_gain).astype(jnp.bfloat16)
    flat_ids = route_ids.reshape(-1)
    onehot = (flat_ids[:, None] == jnp.arange(experts_all, dtype=jnp.int32)[None, :]).astype(
        jnp.int32
    )
    earlier = jnp.cumsum(onehot, axis=0) - onehot
    slot_index = jnp.sum(earlier * onehot, axis=1)
    target = (flat_ids * capacity + slot_index).reshape(row_count, top_count)
    outbound = jnp.zeros((experts_all * capacity, features), jnp.bfloat16)
    for column in range(top_count):
        outbound = outbound.at[target[:, column]].set(normed)
    outbound = outbound.reshape(ep_size, local_experts, capacity, features)
    full_gate, full_up, full_down = (
        lax.all_gather(w_gate, "tp", axis=2, tiled=True),
        lax.all_gather(w_up, "tp", axis=2, tiled=True),
        lax.all_gather(w_down, "tp", axis=1, tiled=True),
    )
    arrived = lax.all_to_all(outbound, "ep", split_axis=0, concat_axis=0, tiled=True)
    gate_pre = jnp.einsum("sjcd,jdf->sjcf", arrived, full_gate, preferred_element_type=jnp.float32)
    up_pre = jnp.einsum("sjcd,jdf->sjcf", arrived, full_up, preferred_element_type=jnp.float32)
    hidden = (jax.nn.silu(gate_pre) * up_pre).astype(jnp.bfloat16)
    result = jnp.einsum("sjcf,jfd->sjcd", hidden, full_down, preferred_element_type=jnp.float32)
    returned_rows = send_back(result.astype(jnp.bfloat16))
    returned_rows = returned_rows.reshape(experts_all * capacity, features)
    combined = jnp.zeros((row_count, features), jnp.float32)
    for column in range(top_count):
        picked = returned_rows[target[:, column]].astype(jnp.float32)
        combined = combined + route_weights[:, column : column + 1] * picked
    return combined.astype(jnp.bfloat16)


def group_kernel(
    members, parts, halves,
    tokens, gain_in, ids_in, weights_in, w_gate, w_up, w_down, out,
    gain, ids, weights, raw, ready, summed, place, sent, taken, scales, scales_in, answers,
    returned, gate_all, up_all, down_all, hidden,
    own_gate, own_up, own_down, extra, extra_scales, partial, parts_out, parts_in,
    raw_sem, small_sems, peer_r, part_r, twin_r, own_r, weight_s, row_s, swap_s, scale_s,
    note_s, back_s, half_s, row_r, extra_r, scale_r, note_r, back_r, half_r,
):
    part, position, half = lax.axis_index("grp"), lax.axis_index("ep"), lax.axis_index("tp")
    level, member = position // members, position % members
    inner = ((level + 1) // 2) % 2
    rows, features = tokens.shape
    slots = sent.shape[1]
    top_count = ids.shape[0]
    peer = {"ep": level * members + (members - 1 - member)}
    other_part = {"grp": parts - 1 - part}
    twin = {"tp": halves - 1 - half}
    slant = {"ep": (level ^ 1) * members + (members - 1 - member)}

    def level_of(k):
        return {"ep": (level ^ k) * members + member}

    on_inner, on_outer = pl.when(inner == 1), pl.when(inner == 0)

    barrier = pltpu.get_barrier_semaphore()
    neighbours = [level_of(k) for k in range(GROUPS - 1, 0, -1)] + [slant, peer, other_part, twin]
    for device in neighbours:
        pl.semaphore_signal(barrier, inc=1, device_id=device, device_id_type=MESH)
    small_copies = [
        pltpu.make_async_copy(src, dst, small_sems.at[i])
        for i, (src, dst) in enumerate(((ids_in, ids), (weights_in, weights), (gain_in, gain)))
    ]
    raw_copy = pltpu.make_async_copy(tokens, raw, raw_sem)
    for copy in small_copies + [raw_copy]:
        copy.start()

    sources = (w_gate, w_up, w_down)
    stores = (gate_all, up_all, down_all)
    own_stores = (own_gate, own_up, own_down)
    mine = member * halves + half
    theirs = (members - 1 - member) * halves + half

    def remote(src, dst, send, recv, device):
        return pltpu.make_async_remote_copy(
            src_ref=src, dst_ref=dst, send_sem=send, recv_sem=recv,
            device_id=device, device_id_type=MESH,
        )

    pieces = [(tensor, step) for step in range(SPLIT) for tensor in range(2)]
    pieces += [(2, step) for step in range(SPLIT)]
    count = len(pieces)
    wide = 2 * SPLIT

    def window_of(piece, which):
        tensor, step = piece
        size = sources[tensor].shape[0] // (parts * SPLIT)
        return pl.ds(pl.multiple_of((which * SPLIT + step) * size, size), size)

    def first_copies(device):
        copies = []
        for i, piece in enumerate(pieces):
            window = window_of(piece, part)
            copies.append(remote(
                sources[piece[0]].at[window], stores[piece[0]].at[mine, window],
                weight_s.at[piece[0]], peer_r.at[i], device,
            ))
        return copies

    def spread_copies(block, which, device):
        copies = []
        for i, piece in enumerate(pieces):
            held = stores[piece[0]].at[block, window_of(piece, which)]
            recv = twin_r.at[piece[0]] if device is twin else part_r.at[i]
            copies.append(remote(held, held, weight_s.at[piece[0]], recv, device))
        return copies

    other = parts - 1 - part
    peer_copies = first_copies(peer)
    part_copies = spread_copies(theirs, part, other_part)
    near_copies = spread_copies(theirs, part, twin)
    far_copies = spread_copies(theirs, other, twin)
    guest_copies = first_copies(level_of(GROUPS - 1))
    cross_copies = spread_copies(mine, part, other_part)
    gnear_copies = spread_copies(mine, part, twin)
    gfar_copies = spread_copies(mine, other, twin)

    def home_copies(targets, block, recv):
        copies, twins = [], []
        for tensor in range(3):
            target = targets[tensor].at[block]
            copies.append(
                pltpu.make_async_copy(sources[tensor], target, small_sems.at[tensor])
            )
            twins.append(
                remote(sources[tensor], target, weight_s.at[tensor], recv.at[tensor], twin)
            )
        return copies, twins

    def block_waits(count):
        waits = []
        for tensor in range(3):
            held = stores[tensor].at[0:count]
            waits.append(remote(held, held, weight_s.at[tensor], twin_r.at[tensor], twin))
        return waits

    group_copies, group_twins = home_copies(stores, mine, twin_r)
    own_copies, own_twins = home_copies(own_stores, half, own_r)
    row_to = {1: level_of(1), 2: level_of(1 + inner), 3: level_of(3)}
    back_to = {1: level_of(1), 2: level_of(2 - inner), 3: level_of(3)}
    tile = features // GROUPS
    tiles = [slice(begin, begin + tile) for begin in range(0, features, tile)]

    def tiled_copies(src, dst, send, recv, base, device):
        return [
            remote(src.at[:, window], dst.at[:, window], send, recv.at[base + t], device)
            for t, window in enumerate(tiles)
        ]

    row_copies, scale_copies = {}, {}
    for k in (1, 2, 3):
        row_copies[k] = remote(sent.at[k], taken.at[k], row_s, row_r.at[k - 1], row_to[k])
        scale_copies[k] = remote(
            scales.at[k, :members], scales_in.at[k, :members],
            scale_s, scale_r.at[k - 1], row_to[k],
        )
    slant_rows = remote(sent.at[1], extra.at[0], row_s, extra_r.at[0], slant)
    slant_scales = remote(
        scales.at[1, :members], extra_scales.at[0, :members], scale_s, note_r.at[0], slant
    )
    back_copies = {
        1: [remote(answers.at[1], returned.at[1], back_s, back_r.at[0], back_to[1])],
        2: tiled_copies(answers.at[2], returned.at[2], back_s, back_r, 1, back_to[2]),
        3: tiled_copies(answers.at[3], returned.at[3], back_s, back_r, 5, back_to[3]),
    }
    swap_copies, note_copies, half_copies = {}, {}, {}
    for j, (buffer, source, k) in enumerate(
        ((taken, scales_in, 0), (taken, scales_in, 2), (sent, scales, 3)), 1
    ):
        swap_copies[j] = remote(buffer.at[k], extra.at[j], swap_s, extra_r.at[j], peer)
        note_copies[j] = remote(
            source.at[k, :members], extra_scales.at[j, :members], note_s, note_r.at[j], peer
        )
    for j, device in ((0, slant), (3, peer)):
        half_copies[j] = [
            remote(parts_out.at[j], parts_in.at[j], half_s, half_r.at[j], device)
        ]
    middle = features // 2
    half_copies[1] = [
        remote(
            parts_out.at[1, :, window], parts_in.at[1, :, window],
            half_s, half_r.at[1 + t], peer,
        )
        for t, window in enumerate((slice(0, middle), slice(middle, features)))
    ]
    half_copies[2] = tiled_copies(parts_out.at[2], parts_in.at[2], half_s, half_r, 4, peer)

    for copy in small_copies:
        copy.wait()
    first = ids[0:1, :]
    group_row = first // members
    lane = lax.broadcasted_iota(jnp.int32, (8, rows), 0)
    mask = (jnp.broadcast_to(group_row, (8, rows)) == lane).astype(jnp.float32)
    before = (
        lax.broadcasted_iota(jnp.int32, (rows, rows), 0)
        < lax.broadcasted_iota(jnp.int32, (rows, rows), 1)
    ).astype(jnp.float32)
    ranks = jnp.dot(
        mask.astype(jnp.bfloat16), before.astype(jnp.bfloat16),
        preferred_element_type=jnp.float32,
    )
    slot_row = jnp.sum(ranks * mask, axis=0, keepdims=True).astype(jnp.int32)
    shares = jnp.zeros((8, rows), jnp.float32)
    for column in range(top_count):
        offset = ids[column : column + 1, :] - group_row * members
        chosen = jnp.broadcast_to(offset, (8, rows)) == lane
        shares = shares + jnp.where(
            chosen, jnp.broadcast_to(weights[column : column + 1, :], (8, rows)), 0.0
        )
    high = shares.astype(jnp.bfloat16)
    rest = shares - high.astype(jnp.float32)
    middle = rest.astype(jnp.bfloat16)
    low = (rest - middle.astype(jnp.float32)).astype(jnp.bfloat16)
    slot_iota = lax.broadcasted_iota(jnp.int32, (slots, rows), 0)

    def pack(k):
        key = jnp.where(group_row == (level ^ k), slot_row, -1)
        spots = (jnp.broadcast_to(key, (slots, rows)) == slot_iota).astype(jnp.float32)
        spots = spots.astype(jnp.bfloat16)
        place[k * slots : (k + 1) * slots, :] = spots
        lanes = sum(
            lax.dot_general(
                piece, spots, (((1,), (1,)), ((), ())), preferred_element_type=jnp.float32
            )
            for piece in (high, middle, low)
        )
        packed = taken if k == 0 else sent
        (scales_in if k == 0 else scales)[k] = lanes
        packed[k] = jnp.dot(spots, raw[...], preferred_element_type=jnp.float32).astype(
            jnp.bfloat16
        )

    def start(copies):
        for copy in copies:
            copy.start()

    def land(copies):
        for copy in copies:
            copy.wait_recv()

    def leave(copies):
        for copy in copies:
            copy.wait_send()

    def swap(j):
        note_copies[j].start()
        swap_copies[j].start()

    def send(k):
        scale_copies[k].start()
        row_copies[k].start()

    def arrive(k):
        land([scale_copies[k], row_copies[k]])

    raw_copy.wait()
    pack(1)
    pl.semaphore_wait(barrier, len(neighbours))

    @on_inner
    def _():
        start(guest_copies)

    send(1)

    @on_outer
    def _():
        slant_scales.start()
        slant_rows.start()
        start(peer_copies)

    pack(0)

    @on_inner
    def _():
        swap(1)
        start(own_copies + own_twins)

    @on_outer
    def _():
        start(group_copies + group_twins)

    pack(2)
    send(2)
    pack(3)

    width = gate_all.shape[2]
    diagonal = lax.broadcasted_iota(jnp.int32, (slots, slots), 0) == lax.broadcasted_iota(
        jnp.int32, (slots, slots), 1
    )
    strip = 32

    def norm(source, base):
        def norm_strip(index, carry):
            start = pl.multiple_of(index * strip, strip)
            floats = source[pl.ds(start, strip), :].astype(jnp.float32)
            inverse = lax.rsqrt(jnp.mean(floats * floats, axis=1, keepdims=True) + epsilon)
            ready[pl.ds(base + start, strip), :] = (floats * inverse * gain[...]).astype(
                jnp.bfloat16
            )
            return carry

        lax.fori_loop(0, slots // strip, norm_strip, 0)

    def column_of(share, owner):
        return jnp.sum(
            jnp.where(diagonal, jnp.broadcast_to(share[pl.ds(owner, 1), :], (slots, slots)), 0.0),
            axis=1, keepdims=True,
        )

    def widen(base, shares_in, owner, gate_block, up_block, column):
        scale = jnp.concatenate([column_of(share, owner) for share in shares_in], axis=0)
        size = slots * len(shares_in)
        values = ready[base : base + size, :]
        gate = jnp.dot(values, gate_block[...], preferred_element_type=jnp.float32)
        up = jnp.dot(values, up_block[...], preferred_element_type=jnp.float32)
        hidden[base : base + size, pl.ds(pl.multiple_of(column * width, width), width)] = (
            gate / (1.0 + jnp.exp(-gate)) * up * scale
        ).astype(jnp.bfloat16)

    def widen_group(base, shares_in, owner, side):
        block = owner * halves + side
        widen(base, shares_in, owner, gate_all.at[block], up_all.at[block], block)

    def narrow(base, size, blocks, column):
        window = slice(column * tile, (column + 1) * tile)
        total = jnp.zeros((size, tile), jnp.float32)
        for index, block in enumerate(blocks):
            total += jnp.dot(
                hidden[base : base + size, index * width : (index + 1) * width],
                block[:, window], preferred_element_type=jnp.float32,
            )
        return window, total

    group_down = [down_all.at[block] for block in range(members * halves)]

    def narrow_group(base, targets):
        for column in range(len(tiles)):
            window, total = narrow(base, slots * len(targets), group_down, column)
            for j, (target, copies) in enumerate(targets):
                target[:, window] = total[j * slots : (j + 1) * slots].astype(jnp.bfloat16)
                if copies and column < len(copies):
                    copies[column].start()

    def whole(ks, held=0):
        for j, k in enumerate(ks):
            norm(taken.at[k], j * slots)
        for owner in range(members):
            for side in range(halves):
                widen_group(0, [scales_in.at[k] for k in ks], owner, side)
        targets = []
        for k in ks:
            ready_tiles = back_copies[k][: len(tiles) - held] if k > 1 else None
            targets.append(((answers if k else returned).at[k], ready_tiles))
        narrow_group(0, targets)
        if 1 in ks:
            back_copies[1][0].start()

    def split(sources_in, gates, ups, downs, store):
        for i, (source, _) in enumerate(sources_in):
            norm(source, i * slots)
        shares_in = [share for _, share in sources_in]
        for side in range(halves):
            widen(0, shares_in, member, gates.at[side], ups.at[side], side)
        blocks = [downs.at[side] for side in range(halves)]
        for column in range(len(tiles)):
            window, total = narrow(0, slots * len(sources_in), blocks, column)
            store(column, window, total)

    def paired(j):
        def store(column, window, total):
            parts_out[j, :, window] = total[:slots].astype(jnp.bfloat16)
            if j == 2:
                half_copies[j][column].start()
            partial[j - 1, :, window] = total[slots:]

        return store

    def joined(j, column, target):
        window = tiles[column]
        target[:, window] = (
            partial[j - 1, :, window] + parts_in[j, :, window].astype(jnp.float32)
        ).astype(jnp.bfloat16)

    def unpack(k, window):
        return lax.dot_general(
            place[k * slots : (k + 1) * slots, :], returned[k, :, window],
            (((0,), (0,)), ((), ())), preferred_element_type=jnp.float32,
        )

    def add(k, fresh=False):
        for window in tiles:
            value = unpack(k, window)
            summed[:, window] = value if fresh else summed[:, window] + value

    def back(k):
        land(back_copies[k])
        add(k)

    def finish(k):
        for t, window in enumerate(tiles):
            back_copies[k][t].wait_recv()
            out[:, window] = (summed[:, window] + unpack(k, window)).astype(jnp.bfloat16)

    def flows(buffer, begin, count, sem):
        held = buffer.at[begin : begin + count]
        return remote(held, held, sem, back_r.at[0], twin)

    def marks(count, sem):
        held = scales.at[0:count, :members]
        return remote(held, held, sem, back_r.at[0], twin)

    @on_outer
    def _():
        for i in range(count):
            peer_copies[i].wait_recv()
            part_copies[i].start()
            near_copies[i].start()
            if i:
                part_copies[i - 1].wait_recv()
                far_copies[i - 1].start()
            if i == LATE:
                send(3)
        part_copies[-1].wait_recv()
        far_copies[-1].start()
        for copy in group_copies:
            copy.wait()
        land(block_waits(2))
        if FIRST:
            arrive(3)
            whole((3,), HELD)
        arrive(1)
        whole((1, 0))
        add(0, True)
        if not FIRST:
            arrive(3)
            whole((3,), HELD)
        arrive(2)
        start(back_copies[3][len(tiles) - HELD :])
        whole((2,))
        back(1)
        half_copies[0][0].wait_recv()
        for window in tiles:
            summed[:, window] = summed[:, window] + lax.dot_general(
                place[slots : 2 * slots, :], parts_in[0, :, window],
                (((0,), (0,)), ((), ())), preferred_element_type=jnp.float32,
            )
        back(2)
        finish(3)
        leave([flows(sent, 0, 4, row_s), marks(4, scale_s), flows(answers, 1, 3, back_s)])

    @on_inner
    def _():
        def take(begin, end):
            for i in range(begin, end):
                guest_copies[i].wait_recv()
                cross_copies[i].start()
                gnear_copies[i].start()
                if i:
                    cross_copies[i - 1].wait_recv()
                    gfar_copies[i - 1].start()

        own = own_stores

        def store_near(column, window, total):
            answers[1, :, window] = total.astype(jnp.bfloat16)

        def store_slant(column, window, total):
            parts_out[0, :, window] = total.astype(jnp.bfloat16)

        take(0, 3)
        for copy in own_copies:
            copy.wait()
        land(own_twins)
        arrive(1)
        split([(taken.at[1], scales_in.at[1])], *own, store_near)
        back_copies[1][0].start()
        take(3, 4)
        land([note_copies[1], swap_copies[1]])
        split([(extra.at[1], extra_scales.at[1]), (taken.at[0], scales_in.at[0])], *own, paired(1))
        swap(3)
        half_copies[1][0].start()
        take(4, 7)
        land([slant_scales, slant_rows])
        split([(extra.at[0], extra_scales.at[0])], *own, store_slant)
        half_copies[0][0].start()
        take(7, 10)
        arrive(2)
        swap(2)
        half_copies[1][1].start()
        take(10, count)
        cross_copies[-1].wait_recv()
        gfar_copies[-1].start()
        land(block_waits(1))
        far = [store.at[pl.ds(member * halves, halves)] for store in stores]
        land([note_copies[2], swap_copies[2]])
        split([(extra.at[2], extra_scales.at[2]), (taken.at[2], scales_in.at[2])], *far, paired(2))
        land([note_copies[3], swap_copies[3]])
        split([(extra.at[3], extra_scales.at[3]), (sent.at[3], scales.at[3])], *far, paired(3))
        half_copies[3][0].start()
        for column in range(len(tiles)):
            half_copies[2][column].wait_recv()
            joined(2, column, answers.at[2])
            back_copies[2][column].start()
        land(half_copies[1])
        for column in range(len(tiles)):
            joined(1, column, returned.at[0])
        add(0, True)
        back(1)
        land(half_copies[3])
        for column in range(len(tiles)):
            joined(3, column, returned.at[3])
        add(3)
        finish(2)
        leave([flows(sent, 0, 2, row_s), marks(2, scale_s), flows(answers, 1, 2, back_s)])
        leave([flows(sent, 0, 3, swap_s), marks(3, note_s), flows(parts_out, 0, 4, half_s)])

    leave(block_waits(3))


def group_layer(members, tokens, norm_gain, route_ids, route_weights, w_gate, w_up, w_down):
    rows, features = tokens.shape
    parts, halves = lax.axis_size("grp"), lax.axis_size("tp")
    width = w_gate.shape[2]
    slots = rows // route_ids.shape[1]
    copies = 3 * SPLIT
    blocks = members * halves
    bf16, f32, dma = jnp.bfloat16, jnp.float32, pltpu.SemaphoreType.DMA

    def vmem(*shape, dtype=bf16):
        return pltpu.VMEM(shape, dtype)

    return pl.pallas_call(
        functools.partial(group_kernel, members, parts, halves),
        out_shape=vmem(rows, features),
        in_specs=[pl.BlockSpec(memory_space=pltpu.HBM)] * 7,
        out_specs=pl.BlockSpec(memory_space=pltpu.VMEM),
        scratch_shapes=[
            vmem(1, features, dtype=f32),
            vmem(*route_ids.shape[::-1], dtype=jnp.int32),
            vmem(*route_ids.shape[::-1], dtype=f32),
            vmem(rows, features),
            vmem(GROUPS * slots, features),
            vmem(rows, features, dtype=f32),
            vmem(GROUPS * slots, rows),
            vmem(GROUPS, slots, features),
            vmem(GROUPS, slots, features),
            vmem(GROUPS, 8, slots, dtype=f32),
            vmem(GROUPS, 8, slots, dtype=f32),
            vmem(GROUPS, slots, features),
            vmem(GROUPS, slots, features),
            vmem(blocks, features, width),
            vmem(blocks, features, width),
            vmem(blocks, width, features),
            vmem(GROUPS * slots, blocks * width),
            vmem(halves, features, width),
            vmem(halves, features, width),
            vmem(halves, width, features),
            vmem(GROUPS, slots, features),
            vmem(GROUPS, 8, slots, dtype=f32),
            vmem(3, slots, features, dtype=f32),
            vmem(GROUPS, slots, features),
            vmem(GROUPS, slots, features),
            dma, dma((3,)), dma((copies,)), dma((copies,)), dma((3,)), dma((3,)), dma((3,)),
            dma, dma, dma, dma, dma, dma, dma((3,)), dma((4,)), dma((3,)), dma((4,)),
            dma((9,)), dma((8,)),
        ],
        compiler_params=pltpu.CompilerParams(
            collective_id=0, has_side_effects=True, vmem_limit_bytes=64400 * 1024
        ),
    )(
        tokens, norm_gain.reshape(1, features), route_ids.T, route_weights.T,
        w_gate[0], w_up[0], w_down[0],
    )


def solution(mesh):
    sizes = mesh.shape

    def per_device(tokens, norm_gain, route_ids, route_weights, w_gate, w_up, w_down):
        arguments = (tokens, norm_gain, route_ids, route_weights, w_gate, w_up, w_down)
        members = sizes["ep"] * w_gate.shape[0] // GROUPS
        paired = members == route_ids.shape[1] == sizes["grp"] == sizes["tp"] == 2
        if paired and w_gate.shape[0] == 1:
            return group_layer(members, *arguments)
        return general_layer(*arguments)

    in_specs = (
        P(("grp", "ep", "tp"), None),
        P(),
        P(("grp", "ep", "tp"), None),
        P(("grp", "ep", "tp"), None),
        P("ep", None, "tp"),
        P("ep", None, "tp"),
        P("ep", "tp", None),
    )
    out_specs = P(("grp", "ep", "tp"), None)
    return jax.shard_map(
        per_device, mesh=mesh, in_specs=in_specs, out_specs=out_specs, check_vma=False
    )
```

```python
import functools

import jax
import jax.numpy as jnp
from jax import lax
from jax.experimental import pallas as pl
from jax.experimental.pallas import tpu as pltpu
from jax.sharding import PartitionSpec as P

GROUPS = 4
SPLIT = 4
HELD = 0
LATE = 7
FIRST = True
MESH = pl.DeviceIdType.MESH


epsilon = 1e-06


def send_back(result):
    return lax.all_to_all(result, "ep", split_axis=0, concat_axis=0, tiled=True)


def general_layer(tokens, norm_gain, route_ids, route_weights, w_gate, w_up, w_down):
    row_count, features = tokens.shape
    top_count = route_ids.shape[1]
    local_experts = w_gate.shape[0]
    ep_size = lax.axis_size("ep")
    experts_all = ep_size * local_experts
    capacity = row_count * GROUPS // experts_all
    floats = tokens.astype(jnp.float32)
    inverse = lax.rsqrt(jnp.mean(floats * floats, axis=1, keepdims=True) + epsilon)
    normed = (floats * inverse * norm_gain).astype(jnp.bfloat16)
    flat_ids = route_ids.reshape(-1)
    onehot = (flat_ids[:, None] == jnp.arange(experts_all, dtype=jnp.int32)[None, :]).astype(
        jnp.int32
    )
    earlier = jnp.cumsum(onehot, axis=0) - onehot
    slot_index = jnp.sum(earlier * onehot, axis=1)
    target = (flat_ids * capacity + slot_index).reshape(row_count, top_count)
    outbound = jnp.zeros((experts_all * capacity, features), jnp.bfloat16)
    for column in range(top_count):
        outbound = outbound.at[target[:, column]].set(normed)
    outbound = outbound.reshape(ep_size, local_experts, capacity, features)
    full_gate, full_up, full_down = (
        lax.all_gather(w_gate, "tp", axis=2, tiled=True),
        lax.all_gather(w_up, "tp", axis=2, tiled=True),
        lax.all_gather(w_down, "tp", axis=1, tiled=True),
    )
    arrived = lax.all_to_all(outbound, "ep", split_axis=0, concat_axis=0, tiled=True)
    gate_pre = jnp.einsum("sjcd,jdf->sjcf", arrived, full_gate, preferred_element_type=jnp.float32)
    up_pre = jnp.einsum("sjcd,jdf->sjcf", arrived, full_up, preferred_element_type=jnp.float32)
    hidden = (jax.nn.silu(gate_pre) * up_pre).astype(jnp.bfloat16)
    result = jnp.einsum("sjcf,jfd->sjcd", hidden, full_down, preferred_element_type=jnp.float32)
    returned_rows = send_back(result.astype(jnp.bfloat16))
    returned_rows = returned_rows.reshape(experts_all * capacity, features)
    combined = jnp.zeros((row_count, features), jnp.float32)
    for column in range(top_count):
        picked = returned_rows[target[:, column]].astype(jnp.float32)
        combined = combined + route_weights[:, column : column + 1] * picked
    return combined.astype(jnp.bfloat16)


def group_kernel(
    members, parts, halves,
    tokens, gain_in, ids_in, weights_in, w_gate, w_up, w_down, out,
    gain, ids, weights, raw, ready, summed, place, sent, taken, scales, scales_in, answers,
    returned, gate_all, up_all, down_all, hidden,
    own_gate, own_up, own_down, extra, extra_scales, partial, parts_out, parts_in,
    raw_sem, small_sems, peer_r, part_r, twin_r, own_r, weight_s, row_s, swap_s, scale_s,
    note_s, back_s, half_s, row_r, extra_r, scale_r, note_r, back_r, half_r,
):
    part, position, half = lax.axis_index("grp"), lax.axis_index("ep"), lax.axis_index("tp")
    level, member = position // members, position % members
    inner = ((level + 1) // 2) % 2
    rows, features = tokens.shape
    slots = sent.shape[1]
    top_count = ids.shape[0]
    peer = {"ep": level * members + (members - 1 - member)}
    other_part = {"grp": parts - 1 - part}
    twin = {"tp": halves - 1 - half}
    slant = {"ep": (level ^ 1) * members + (members - 1 - member)}

    def level_of(k):
        return {"ep": (level ^ k) * members + member}

    on_inner, on_outer = pl.when(inner == 1), pl.when(inner == 0)

    barrier = pltpu.get_barrier_semaphore()
    neighbours = [level_of(k) for k in range(GROUPS - 1, 0, -1)] + [slant, peer, other_part, twin]
    for device in neighbours:
        pl.semaphore_signal(barrier, inc=1, device_id=device, device_id_type=MESH)
    small_copies = [
        pltpu.make_async_copy(src, dst, small_sems.at[i])
        for i, (src, dst) in enumerate(((ids_in, ids), (weights_in, weights), (gain_in, gain)))
    ]
    raw_copy = pltpu.make_async_copy(tokens, raw, raw_sem)
    for copy in small_copies + [raw_copy]:
        copy.start()

    sources = (w_gate, w_up, w_down)
    stores = (gate_all, up_all, down_all)
    own_stores = (own_gate, own_up, own_down)
    mine = member * halves + half
    theirs = (members - 1 - member) * halves + half

    def remote(src, dst, send, recv, device):
        return pltpu.make_async_remote_copy(
            src_ref=src, dst_ref=dst, send_sem=send, recv_sem=recv,
            device_id=device, device_id_type=MESH,
        )

    pieces = [(tensor, step) for step in range(SPLIT) for tensor in range(2)]
    pieces += [(2, step) for step in range(SPLIT)]
    count = len(pieces)
    wide = 2 * SPLIT

    def window_of(piece, which):
        tensor, step = piece
        size = sources[tensor].shape[0] // (parts * SPLIT)
        return pl.ds(pl.multiple_of((which * SPLIT + step) * size, size), size)

    def first_copies(device):
        copies = []
        for i, piece in enumerate(pieces):
            window = window_of(piece, part)
            copies.append(remote(
                sources[piece[0]].at[window], stores[piece[0]].at[mine, window],
                weight_s.at[piece[0]], peer_r.at[i], device,
            ))
        return copies

    def spread_copies(block, which, device):
        copies = []
        for i, piece in enumerate(pieces):
            held = stores[piece[0]].at[block, window_of(piece, which)]
            recv = twin_r.at[piece[0]] if device is twin else part_r.at[i]
            copies.append(remote(held, held, weight_s.at[piece[0]], recv, device))
        return copies

    other = parts - 1 - part
    peer_copies = first_copies(peer)
    part_copies = spread_copies(theirs, part, other_part)
    near_copies = spread_copies(theirs, part, twin)
    far_copies = spread_copies(theirs, other, twin)
    guest_copies = first_copies(level_of(GROUPS - 1))
    cross_copies = spread_copies(mine, part, other_part)
    gnear_copies = spread_copies(mine, part, twin)
    gfar_copies = spread_copies(mine, other, twin)

    def home_copies(targets, block, recv):
        copies, twins = [], []
        for tensor in range(3):
            target = targets[tensor].at[block]
            copies.append(
                pltpu.make_async_copy(sources[tensor], target, small_sems.at[tensor])
            )
            twins.append(
                remote(sources[tensor], target, weight_s.at[tensor], recv.at[tensor], twin)
            )
        return copies, twins

    def block_waits(count):
        waits = []
        for tensor in range(3):
            held = stores[tensor].at[0:count]
            waits.append(remote(held, held, weight_s.at[tensor], twin_r.at[tensor], twin))
        return waits

    group_copies, group_twins = home_copies(stores, mine, twin_r)
    own_copies, own_twins = home_copies(own_stores, half, own_r)
    row_to = {1: level_of(1), 2: level_of(1 + inner), 3: level_of(3)}
    back_to = {1: level_of(1), 2: level_of(2 - inner), 3: level_of(3)}
    tile = features // GROUPS
    tiles = [slice(begin, begin + tile) for begin in range(0, features, tile)]

    def tiled_copies(src, dst, send, recv, base, device):
        return [
            remote(src.at[:, window], dst.at[:, window], send, recv.at[base + t], device)
            for t, window in enumerate(tiles)
        ]

    row_copies, scale_copies = {}, {}
    for k in (1, 2, 3):
        row_copies[k] = remote(sent.at[k], taken.at[k], row_s, row_r.at[k - 1], row_to[k])
        scale_copies[k] = remote(
            scales.at[k, :members], scales_in.at[k, :members],
            scale_s, scale_r.at[k - 1], row_to[k],
        )
    slant_rows = remote(sent.at[1], extra.at[0], row_s, extra_r.at[0], slant)
    slant_scales = remote(
        scales.at[1, :members], extra_scales.at[0, :members], scale_s, note_r.at[0], slant
    )
    back_copies = {
        1: [remote(answers.at[1], returned.at[1], back_s, back_r.at[0], back_to[1])],
        2: tiled_copies(answers.at[2], returned.at[2], back_s, back_r, 1, back_to[2]),
        3: tiled_copies(answers.at[3], returned.at[3], back_s, back_r, 5, back_to[3]),
    }
    swap_copies, note_copies, half_copies = {}, {}, {}
    for j, (buffer, source, k) in enumerate(
        ((taken, scales_in, 0), (taken, scales_in, 2), (sent, scales, 3)), 1
    ):
        swap_copies[j] = remote(buffer.at[k], extra.at[j], swap_s, extra_r.at[j], peer)
        note_copies[j] = remote(
            source.at[k, :members], extra_scales.at[j, :members], note_s, note_r.at[j], peer
        )
    for j, device in ((0, slant), (3, peer)):
        half_copies[j] = [
            remote(parts_out.at[j], parts_in.at[j], half_s, half_r.at[j], device)
        ]
    middle = features // 2
    half_copies[1] = [
        remote(
            parts_out.at[1, :, window], parts_in.at[1, :, window],
            half_s, half_r.at[1 + t], peer,
        )
        for t, window in enumerate((slice(0, middle), slice(middle, features)))
    ]
    half_copies[2] = tiled_copies(parts_out.at[2], parts_in.at[2], half_s, half_r, 4, peer)

    for copy in small_copies:
        copy.wait()
    first = ids[0:1, :]
    group_row = first // members
    lane = lax.broadcasted_iota(jnp.int32, (8, rows), 0)
    mask = (jnp.broadcast_to(group_row, (8, rows)) == lane).astype(jnp.float32)
    before = (
        lax.broadcasted_iota(jnp.int32, (rows, rows), 0)
        < lax.broadcasted_iota(jnp.int32, (rows, rows), 1)
    ).astype(jnp.float32)
    ranks = jnp.dot(
        mask.astype(jnp.bfloat16), before.astype(jnp.bfloat16),
        preferred_element_type=jnp.float32,
    )
    slot_row = jnp.sum(ranks * mask, axis=0, keepdims=True).astype(jnp.int32)
    shares = jnp.zeros((8, rows), jnp.float32)
    for column in range(top_count):
        offset = ids[column : column + 1, :] - group_row * members
        chosen = jnp.broadcast_to(offset, (8, rows)) == lane
        shares = shares + jnp.where(
            chosen, jnp.broadcast_to(weights[column : column + 1, :], (8, rows)), 0.0
        )
    high = shares.astype(jnp.bfloat16)
    rest = shares - high.astype(jnp.float32)
    middle = rest.astype(jnp.bfloat16)
    low = (rest - middle.astype(jnp.float32)).astype(jnp.bfloat16)
    slot_iota = lax.broadcasted_iota(jnp.int32, (slots, rows), 0)

    def pack(k):
        key = jnp.where(group_row == (level ^ k), slot_row, -1)
        spots = (jnp.broadcast_to(key, (slots, rows)) == slot_iota).astype(jnp.float32)
        spots = spots.astype(jnp.bfloat16)
        place[k * slots : (k + 1) * slots, :] = spots
        lanes = sum(
            lax.dot_general(
                piece, spots, (((1,), (1,)), ((), ())), preferred_element_type=jnp.float32
            )
            for piece in (high, middle, low)
        )
        packed = taken if k == 0 else sent
        (scales_in if k == 0 else scales)[k] = lanes
        packed[k] = jnp.dot(spots, raw[...], preferred_element_type=jnp.float32).astype(
            jnp.bfloat16
        )

    def start(copies):
        for copy in copies:
            copy.start()

    def land(copies):
        for copy in copies:
            copy.wait_recv()

    def leave(copies):
        for copy in copies:
            copy.wait_send()

    def swap(j):
        note_copies[j].start()
        swap_copies[j].start()

    def send(k):
        scale_copies[k].start()
        row_copies[k].start()

    def arrive(k):
        land([scale_copies[k], row_copies[k]])

    raw_copy.wait()
    pack(1)
    pl.semaphore_wait(barrier, len(neighbours))

    @on_inner
    def _():
        start(guest_copies)

    @on_outer
    def _():
        start(peer_copies)

    send(1)

    @on_outer
    def _():
        slant_scales.start()
        slant_rows.start()

    pack(0)

    @on_inner
    def _():
        swap(1)
        start(own_copies + own_twins)

    @on_outer
    def _():
        start(group_copies + group_twins)

    pack(2)
    send(2)
    pack(3)

    width = gate_all.shape[2]
    diagonal = lax.broadcasted_iota(jnp.int32, (slots, slots), 0) == lax.broadcasted_iota(
        jnp.int32, (slots, slots), 1
    )
    strip = 32

    def norm(source, base):
        def norm_strip(index, carry):
            start = pl.multiple_of(index * strip, strip)
            floats = source[pl.ds(start, strip), :].astype(jnp.float32)
            inverse = lax.rsqrt(jnp.mean(floats * floats, axis=1, keepdims=True) + epsilon)
            ready[pl.ds(base + start, strip), :] = (floats * inverse * gain[...]).astype(
                jnp.bfloat16
            )
            return carry

        lax.fori_loop(0, slots // strip, norm_strip, 0)

    def column_of(share, owner):
        return jnp.sum(
            jnp.where(diagonal, jnp.broadcast_to(share[pl.ds(owner, 1), :], (slots, slots)), 0.0),
            axis=1, keepdims=True,
        )

    def widen(base, shares_in, owner, gate_block, up_block, column):
        scale = jnp.concatenate([column_of(share, owner) for share in shares_in], axis=0)
        size = slots * len(shares_in)
        values = ready[base : base + size, :]
        gate = jnp.dot(values, gate_block[...], preferred_element_type=jnp.float32)
        up = jnp.dot(values, up_block[...], preferred_element_type=jnp.float32)
        hidden[base : base + size, pl.ds(pl.multiple_of(column * width, width), width)] = (
            gate / (1.0 + jnp.exp(-gate)) * up * scale
        ).astype(jnp.bfloat16)

    def widen_group(base, shares_in, owner, side):
        block = owner * halves + side
        widen(base, shares_in, owner, gate_all.at[block], up_all.at[block], block)

    def narrow(base, size, blocks, column):
        window = slice(column * tile, (column + 1) * tile)
        total = jnp.zeros((size, tile), jnp.float32)
        for index, block in enumerate(blocks):
            total += jnp.dot(
                hidden[base : base + size, index * width : (index + 1) * width],
                block[:, window], preferred_element_type=jnp.float32,
            )
        return window, total

    group_down = [down_all.at[block] for block in range(members * halves)]

    def narrow_group(base, targets):
        for column in range(len(tiles)):
            window, total = narrow(base, slots * len(targets), group_down, column)
            for j, (target, copies) in enumerate(targets):
                target[:, window] = total[j * slots : (j + 1) * slots].astype(jnp.bfloat16)
                if copies and column < len(copies):
                    copies[column].start()

    def whole(ks, held=0):
        for j, k in enumerate(ks):
            norm(taken.at[k], j * slots)
        for owner in range(members):
            for side in range(halves):
                widen_group(0, [scales_in.at[k] for k in ks], owner, side)
        targets = []
        for k in ks:
            ready_tiles = back_copies[k][: len(tiles) - held] if k > 1 else None
            targets.append(((answers if k else returned).at[k], ready_tiles))
        narrow_group(0, targets)
        if 1 in ks:
            back_copies[1][0].start()

    def split(sources_in, gates, ups, downs, store):
        for i, (source, _) in enumerate(sources_in):
            norm(source, i * slots)
        shares_in = [share for _, share in sources_in]
        for side in range(halves):
            widen(0, shares_in, member, gates.at[side], ups.at[side], side)
        blocks = [downs.at[side] for side in range(halves)]
        for column in range(len(tiles)):
            window, total = narrow(0, slots * len(sources_in), blocks, column)
            store(column, window, total)

    def paired(j):
        def store(column, window, total):
            parts_out[j, :, window] = total[:slots].astype(jnp.bfloat16)
            if j == 2:
                half_copies[j][column].start()
            partial[j - 1, :, window] = total[slots:]

        return store

    def joined(j, column, target):
        window = tiles[column]
        target[:, window] = (
            partial[j - 1, :, window] + parts_in[j, :, window].astype(jnp.float32)
        ).astype(jnp.bfloat16)

    def unpack(k, window):
        return lax.dot_general(
            place[k * slots : (k + 1) * slots, :], returned[k, :, window],
            (((0,), (0,)), ((), ())), preferred_element_type=jnp.float32,
        )

    def add(k, fresh=False):
        for window in tiles:
            value = unpack(k, window)
            summed[:, window] = value if fresh else summed[:, window] + value

    def back(k):
        land(back_copies[k])
        add(k)

    def finish(k):
        for t, window in enumerate(tiles):
            back_copies[k][t].wait_recv()
            out[:, window] = (summed[:, window] + unpack(k, window)).astype(jnp.bfloat16)

    def flows(buffer, begin, count, sem):
        held = buffer.at[begin : begin + count]
        return remote(held, held, sem, back_r.at[0], twin)

    def marks(count, sem):
        held = scales.at[0:count, :members]
        return remote(held, held, sem, back_r.at[0], twin)

    @on_outer
    def _():
        for i in range(count):
            peer_copies[i].wait_recv()
            part_copies[i].start()
            near_copies[i].start()
            if i:
                part_copies[i - 1].wait_recv()
                far_copies[i - 1].start()
            if i == LATE:
                send(3)
        part_copies[-1].wait_recv()
        far_copies[-1].start()
        for copy in group_copies:
            copy.wait()
        land(block_waits(2))
        if FIRST:
            arrive(3)
            whole((3,), HELD)
        arrive(1)
        whole((1, 0))
        add(0, True)
        if not FIRST:
            arrive(3)
            whole((3,), HELD)
        arrive(2)
        start(back_copies[3][len(tiles) - HELD :])
        whole((2,))
        back(1)
        half_copies[0][0].wait_recv()
        for window in tiles:
            summed[:, window] = summed[:, window] + lax.dot_general(
                place[slots : 2 * slots, :], parts_in[0, :, window],
                (((0,), (0,)), ((), ())), preferred_element_type=jnp.float32,
            )
        for t, window in enumerate(tiles):
            land([back_copies[3][t], back_copies[2][t]])
            pair = returned[2:4, :, window].reshape(2 * slots, tile)
            total = summed[:, window] + lax.dot_general(
                place[2 * slots : 4 * slots, :], pair,
                (((0,), (0,)), ((), ())), preferred_element_type=jnp.float32,
            )
            out[:, window] = total.astype(jnp.bfloat16)
        leave([flows(sent, 0, 4, row_s), marks(4, scale_s), flows(answers, 1, 3, back_s)])

    @on_inner
    def _():
        def take(begin, end):
            for i in range(begin, end):
                guest_copies[i].wait_recv()
                cross_copies[i].start()
                gnear_copies[i].start()
                if i:
                    cross_copies[i - 1].wait_recv()
                    gfar_copies[i - 1].start()

        own = own_stores

        def store_near(column, window, total):
            answers[1, :, window] = total.astype(jnp.bfloat16)

        def store_slant(column, window, total):
            parts_out[0, :, window] = total.astype(jnp.bfloat16)

        take(0, 3)
        for copy in own_copies:
            copy.wait()
        land(own_twins)
        arrive(1)
        split([(taken.at[1], scales_in.at[1])], *own, store_near)
        back_copies[1][0].start()
        take(3, 4)
        land([note_copies[1], swap_copies[1]])
        split([(extra.at[1], extra_scales.at[1]), (taken.at[0], scales_in.at[0])], *own, paired(1))
        swap(3)
        half_copies[1][0].start()
        take(4, 7)
        land([slant_scales, slant_rows])
        split([(extra.at[0], extra_scales.at[0])], *own, store_slant)
        half_copies[0][0].start()
        take(7, 10)
        arrive(2)
        swap(2)
        half_copies[1][1].start()
        take(10, count)
        cross_copies[-1].wait_recv()
        gfar_copies[-1].start()
        land(block_waits(1))
        far = [store.at[pl.ds(member * halves, halves)] for store in stores]
        land([note_copies[2], swap_copies[2]])
        split([(extra.at[2], extra_scales.at[2]), (taken.at[2], scales_in.at[2])], *far, paired(2))
        land([note_copies[3], swap_copies[3]])
        split([(extra.at[3], extra_scales.at[3]), (sent.at[3], scales.at[3])], *far, paired(3))
        half_copies[3][0].start()
        for column in range(len(tiles)):
            half_copies[2][column].wait_recv()
            joined(2, column, answers.at[2])
            back_copies[2][column].start()
        land(half_copies[1])
        for column in range(len(tiles)):
            joined(1, column, returned.at[0])
        add(0, True)
        back(1)
        land(half_copies[3])
        for column in range(len(tiles)):
            joined(3, column, returned.at[3])
        add(3)
        finish(2)
        leave([flows(sent, 0, 2, row_s), marks(2, scale_s), flows(answers, 1, 2, back_s)])
        leave([flows(sent, 0, 3, swap_s), marks(3, note_s), flows(parts_out, 0, 4, half_s)])

    leave(block_waits(3))


def group_layer(members, tokens, norm_gain, route_ids, route_weights, w_gate, w_up, w_down):
    rows, features = tokens.shape
    parts, halves = lax.axis_size("grp"), lax.axis_size("tp")
    width = w_gate.shape[2]
    slots = rows // route_ids.shape[1]
    copies = 3 * SPLIT
    blocks = members * halves
    bf16, f32, dma = jnp.bfloat16, jnp.float32, pltpu.SemaphoreType.DMA

    def vmem(*shape, dtype=bf16):
        return pltpu.VMEM(shape, dtype)

    return pl.pallas_call(
        functools.partial(group_kernel, members, parts, halves),
        out_shape=vmem(rows, features),
        in_specs=[pl.BlockSpec(memory_space=pltpu.HBM)] * 7,
        out_specs=pl.BlockSpec(memory_space=pltpu.VMEM),
        scratch_shapes=[
            vmem(1, features, dtype=f32),
            vmem(*route_ids.shape[::-1], dtype=jnp.int32),
            vmem(*route_ids.shape[::-1], dtype=f32),
            vmem(rows, features),
            vmem(GROUPS * slots, features),
            vmem(rows, features, dtype=f32),
            vmem(GROUPS * slots, rows),
            vmem(GROUPS, slots, features),
            vmem(GROUPS, slots, features),
            vmem(GROUPS, 8, slots, dtype=f32),
            vmem(GROUPS, 8, slots, dtype=f32),
            vmem(GROUPS, slots, features),
            vmem(GROUPS, slots, features),
            vmem(blocks, features, width),
            vmem(blocks, features, width),
            vmem(blocks, width, features),
            vmem(GROUPS * slots, blocks * width),
            vmem(halves, features, width),
            vmem(halves, features, width),
            vmem(halves, width, features),
            vmem(GROUPS, slots, features),
            vmem(GROUPS, 8, slots, dtype=f32),
            vmem(3, slots, features, dtype=f32),
            vmem(GROUPS, slots, features),
            vmem(GROUPS, slots, features),
            dma, dma((3,)), dma((copies,)), dma((copies,)), dma((3,)), dma((3,)), dma((3,)),
            dma, dma, dma, dma, dma, dma, dma((3,)), dma((4,)), dma((3,)), dma((4,)),
            dma((9,)), dma((8,)),
        ],
        compiler_params=pltpu.CompilerParams(
            collective_id=0, has_side_effects=True, vmem_limit_bytes=64400 * 1024
        ),
    )(
        tokens, norm_gain.reshape(1, features), route_ids.T, route_weights.T,
        w_gate[0], w_up[0], w_down[0],
    )


def solution(mesh):
    sizes = mesh.shape

    def per_device(tokens, norm_gain, route_ids, route_weights, w_gate, w_up, w_down):
        arguments = (tokens, norm_gain, route_ids, route_weights, w_gate, w_up, w_down)
        members = sizes["ep"] * w_gate.shape[0] // GROUPS
        paired = members == route_ids.shape[1] == sizes["grp"] == sizes["tp"] == 2
        if paired and w_gate.shape[0] == 1:
            return group_layer(members, *arguments)
        return general_layer(*arguments)

    in_specs = (
        P(("grp", "ep", "tp"), None),
        P(),
        P(("grp", "ep", "tp"), None),
        P(("grp", "ep", "tp"), None),
        P("ep", None, "tp"),
        P("ep", None, "tp"),
        P("ep", "tp", None),
    )
    out_specs = P(("grp", "ep", "tp"), None)
    return jax.shard_map(
        per_device, mesh=mesh, in_specs=in_specs, out_specs=out_specs, check_vma=False
    )
```

```python
import functools

import jax
import jax.numpy as jnp
from jax import lax
from jax.experimental import pallas as pl
from jax.experimental.pallas import tpu as pltpu
from jax.sharding import PartitionSpec as P

GROUPS = 4
SPLIT = 4
LATE = 7
MESH = pl.DeviceIdType.MESH


epsilon = 1e-06


def send_back(result):
    return lax.all_to_all(result, "ep", split_axis=0, concat_axis=0, tiled=True)


def general_layer(tokens, norm_gain, route_ids, route_weights, w_gate, w_up, w_down):
    row_count, features = tokens.shape
    top_count = route_ids.shape[1]
    local_experts = w_gate.shape[0]
    ep_size = lax.axis_size("ep")
    experts_all = ep_size * local_experts
    capacity = row_count * GROUPS // experts_all
    floats = tokens.astype(jnp.float32)
    inverse = lax.rsqrt(jnp.mean(floats * floats, axis=1, keepdims=True) + epsilon)
    normed = (floats * inverse * norm_gain).astype(jnp.bfloat16)
    flat_ids = route_ids.reshape(-1)
    onehot = (flat_ids[:, None] == jnp.arange(experts_all, dtype=jnp.int32)[None, :]).astype(
        jnp.int32
    )
    earlier = jnp.cumsum(onehot, axis=0) - onehot
    slot_index = jnp.sum(earlier * onehot, axis=1)
    target = (flat_ids * capacity + slot_index).reshape(row_count, top_count)
    outbound = jnp.zeros((experts_all * capacity, features), jnp.bfloat16)
    for column in range(top_count):
        outbound = outbound.at[target[:, column]].set(normed)
    outbound = outbound.reshape(ep_size, local_experts, capacity, features)
    full_gate, full_up, full_down = (
        lax.all_gather(w_gate, "tp", axis=2, tiled=True),
        lax.all_gather(w_up, "tp", axis=2, tiled=True),
        lax.all_gather(w_down, "tp", axis=1, tiled=True),
    )
    arrived = lax.all_to_all(outbound, "ep", split_axis=0, concat_axis=0, tiled=True)
    gate_pre = jnp.einsum("sjcd,jdf->sjcf", arrived, full_gate, preferred_element_type=jnp.float32)
    up_pre = jnp.einsum("sjcd,jdf->sjcf", arrived, full_up, preferred_element_type=jnp.float32)
    hidden = (jax.nn.silu(gate_pre) * up_pre).astype(jnp.bfloat16)
    result = jnp.einsum("sjcf,jfd->sjcd", hidden, full_down, preferred_element_type=jnp.float32)
    returned_rows = send_back(result.astype(jnp.bfloat16))
    returned_rows = returned_rows.reshape(experts_all * capacity, features)
    combined = jnp.zeros((row_count, features), jnp.float32)
    for column in range(top_count):
        picked = returned_rows[target[:, column]].astype(jnp.float32)
        combined = combined + route_weights[:, column : column + 1] * picked
    return combined.astype(jnp.bfloat16)


def group_kernel(
    members, parts, halves,
    tokens, gain_in, ids_in, weights_in, w_gate, w_up, w_down, out,
    gain, ids, weights, raw, ready, summed, place, sent, taken, scales, scales_in, answers,
    returned, gate_all, up_all, down_all, hidden,
    own_gate, own_up, own_down, extra, extra_scales, partial, parts_out, parts_in,
    raw_sem, small_sems, peer_r, part_r, twin_r, own_r, weight_s, row_s, swap_s, scale_s,
    note_s, back_s, half_s, row_r, extra_r, scale_r, note_r, back_r, half_r,
):
    part, position, half = lax.axis_index("grp"), lax.axis_index("ep"), lax.axis_index("tp")
    level, member = position // members, position % members
    inner = ((level + 1) // 2) % 2
    rows, features = tokens.shape
    slots = sent.shape[1]
    top_count = ids.shape[0]
    peer = {"ep": level * members + (members - 1 - member)}
    other_part = {"grp": parts - 1 - part}
    twin = {"tp": halves - 1 - half}
    slant = {"ep": (level ^ 1) * members + (members - 1 - member)}

    def level_of(k):
        return {"ep": (level ^ k) * members + member}

    on_inner, on_outer = pl.when(inner == 1), pl.when(inner == 0)

    barrier = pltpu.get_barrier_semaphore()
    neighbours = [level_of(k) for k in range(GROUPS - 1, 0, -1)] + [slant, peer, other_part, twin]
    for device in neighbours:
        pl.semaphore_signal(barrier, inc=1, device_id=device, device_id_type=MESH)
    small_copies = [
        pltpu.make_async_copy(src, dst, small_sems.at[i])
        for i, (src, dst) in enumerate(((ids_in, ids), (weights_in, weights), (gain_in, gain)))
    ]
    raw_copy = pltpu.make_async_copy(tokens, raw, raw_sem)
    for copy in small_copies + [raw_copy]:
        copy.start()

    sources = (w_gate, w_up, w_down)
    stores = (gate_all, up_all, down_all)
    own_stores = (own_gate, own_up, own_down)
    mine = member * halves + half
    theirs = (members - 1 - member) * halves + half

    def remote(src, dst, send, recv, device):
        return pltpu.make_async_remote_copy(
            src_ref=src, dst_ref=dst, send_sem=send, recv_sem=recv,
            device_id=device, device_id_type=MESH,
        )

    pieces = [(tensor, step) for step in range(SPLIT) for tensor in range(2)]
    pieces += [(2, step) for step in range(SPLIT)]
    count = len(pieces)
    wide = 2 * SPLIT

    def window_of(piece, which):
        tensor, step = piece
        size = sources[tensor].shape[0] // (parts * SPLIT)
        return pl.ds(pl.multiple_of((which * SPLIT + step) * size, size), size)

    def first_copies(device):
        copies = []
        for i, piece in enumerate(pieces):
            window = window_of(piece, part)
            copies.append(remote(
                sources[piece[0]].at[window], stores[piece[0]].at[mine, window],
                weight_s.at[piece[0]], peer_r.at[i], device,
            ))
        return copies

    def spread_copies(block, which, device):
        copies = []
        for i, piece in enumerate(pieces):
            held = stores[piece[0]].at[block, window_of(piece, which)]
            recv = twin_r.at[piece[0]] if device is twin else part_r.at[i]
            copies.append(remote(held, held, weight_s.at[piece[0]], recv, device))
        return copies

    other = parts - 1 - part
    peer_copies = first_copies(peer)
    part_copies = spread_copies(theirs, part, other_part)
    near_copies = spread_copies(theirs, part, twin)
    far_copies = spread_copies(theirs, other, twin)
    guest_copies = first_copies(level_of(GROUPS - 1))
    cross_copies = spread_copies(mine, part, other_part)
    gnear_copies = spread_copies(mine, part, twin)
    gfar_copies = spread_copies(mine, other, twin)

    def home_copies(targets, block, recv):
        copies, twins = [], []
        for tensor in range(3):
            target = targets[tensor].at[block]
            copies.append(
                pltpu.make_async_copy(sources[tensor], target, small_sems.at[tensor])
            )
            twins.append(
                remote(sources[tensor], target, weight_s.at[tensor], recv.at[tensor], twin)
            )
        return copies, twins

    def block_waits(count):
        waits = []
        for tensor in range(3):
            held = stores[tensor].at[0:count]
            waits.append(remote(held, held, weight_s.at[tensor], twin_r.at[tensor], twin))
        return waits

    group_copies, group_twins = home_copies(stores, mine, twin_r)
    own_copies, own_twins = home_copies(own_stores, half, own_r)
    row_to = {1: level_of(1), 2: level_of(1 + inner), 3: level_of(3)}
    back_to = {1: level_of(1), 2: level_of(2 - inner), 3: level_of(3)}
    tile = features // GROUPS
    tiles = [slice(begin, begin + tile) for begin in range(0, features, tile)]

    def tiled_copies(src, dst, send, recv, base, device):
        return [
            remote(src.at[:, window], dst.at[:, window], send, recv.at[base + t], device)
            for t, window in enumerate(tiles)
        ]

    row_copies, scale_copies = {}, {}
    for k in (1, 2, 3):
        row_copies[k] = remote(sent.at[k], taken.at[k], row_s, row_r.at[k - 1], row_to[k])
        scale_copies[k] = remote(
            scales.at[k, :members], scales_in.at[k, :members],
            scale_s, scale_r.at[k - 1], row_to[k],
        )
    slant_rows = remote(sent.at[1], extra.at[0], row_s, extra_r.at[0], slant)
    slant_scales = remote(
        scales.at[1, :members], extra_scales.at[0, :members], scale_s, note_r.at[0], slant
    )
    back_copies = {
        1: [remote(answers.at[1], returned.at[1], back_s, back_r.at[0], back_to[1])],
        2: tiled_copies(answers.at[2], returned.at[2], back_s, back_r, 1, back_to[2]),
        3: tiled_copies(answers.at[3], returned.at[3], back_s, back_r, 5, back_to[3]),
    }
    swap_copies, note_copies, half_copies = {}, {}, {}
    for j, (buffer, source, k) in enumerate(
        ((taken, scales_in, 0), (taken, scales_in, 2), (sent, scales, 3)), 1
    ):
        swap_copies[j] = remote(buffer.at[k], extra.at[j], swap_s, extra_r.at[j], peer)
        note_copies[j] = remote(
            source.at[k, :members], extra_scales.at[j, :members], note_s, note_r.at[j], peer
        )
    for j, device in ((0, slant), (3, peer)):
        half_copies[j] = [
            remote(parts_out.at[j], parts_in.at[j], half_s, half_r.at[j], device)
        ]
    middle = features // 2
    half_copies[1] = [
        remote(
            parts_out.at[1, :, window], parts_in.at[1, :, window],
            half_s, half_r.at[1 + t], peer,
        )
        for t, window in enumerate((slice(0, middle), slice(middle, features)))
    ]
    half_copies[2] = tiled_copies(parts_out.at[2], parts_in.at[2], half_s, half_r, 4, peer)

    for copy in small_copies:
        copy.wait()
    first = ids[0:1, :]
    group_row = first // members
    lane = lax.broadcasted_iota(jnp.int32, (8, rows), 0)
    mask = (jnp.broadcast_to(group_row, (8, rows)) == lane).astype(jnp.float32)
    before = (
        lax.broadcasted_iota(jnp.int32, (rows, rows), 0)
        < lax.broadcasted_iota(jnp.int32, (rows, rows), 1)
    ).astype(jnp.float32)
    ranks = jnp.dot(
        mask.astype(jnp.bfloat16), before.astype(jnp.bfloat16),
        preferred_element_type=jnp.float32,
    )
    slot_row = jnp.sum(ranks * mask, axis=0, keepdims=True).astype(jnp.int32)
    shares = jnp.zeros((8, rows), jnp.float32)
    for column in range(top_count):
        offset = ids[column : column + 1, :] - group_row * members
        chosen = jnp.broadcast_to(offset, (8, rows)) == lane
        shares = shares + jnp.where(
            chosen, jnp.broadcast_to(weights[column : column + 1, :], (8, rows)), 0.0
        )
    high = shares.astype(jnp.bfloat16)
    rest = shares - high.astype(jnp.float32)
    middle = rest.astype(jnp.bfloat16)
    low = (rest - middle.astype(jnp.float32)).astype(jnp.bfloat16)
    slot_iota = lax.broadcasted_iota(jnp.int32, (slots, rows), 0)

    def pack(k):
        key = jnp.where(group_row == (level ^ k), slot_row, -1)
        spots = (jnp.broadcast_to(key, (slots, rows)) == slot_iota).astype(jnp.float32)
        spots = spots.astype(jnp.bfloat16)
        place[k * slots : (k + 1) * slots, :] = spots
        lanes = sum(
            lax.dot_general(
                piece, spots, (((1,), (1,)), ((), ())), preferred_element_type=jnp.float32
            )
            for piece in (high, middle, low)
        )
        packed = taken if k == 0 else sent
        (scales_in if k == 0 else scales)[k] = lanes
        packed[k] = jnp.dot(spots, raw[...], preferred_element_type=jnp.float32).astype(
            jnp.bfloat16
        )

    def start(copies):
        for copy in copies:
            copy.start()

    def land(copies):
        for copy in copies:
            copy.wait_recv()

    def leave(copies):
        for copy in copies:
            copy.wait_send()

    def swap(j):
        note_copies[j].start()
        swap_copies[j].start()

    def send(k):
        scale_copies[k].start()
        row_copies[k].start()

    def arrive(k):
        land([scale_copies[k], row_copies[k]])

    raw_copy.wait()
    pack(1)
    pl.semaphore_wait(barrier, len(neighbours))

    @on_inner
    def _():
        start(guest_copies)

    @on_outer
    def _():
        start(peer_copies)

    send(1)

    @on_outer
    def _():
        slant_scales.start()
        slant_rows.start()

    pack(0)

    @on_inner
    def _():
        swap(1)
        start(own_copies + own_twins)

    @on_outer
    def _():
        start(group_copies + group_twins)

    pack(2)
    send(2)
    pack(3)

    width = gate_all.shape[2]
    diagonal = lax.broadcasted_iota(jnp.int32, (slots, slots), 0) == lax.broadcasted_iota(
        jnp.int32, (slots, slots), 1
    )
    strip = 32

    def norm(source, base):
        def norm_strip(index, carry):
            start = pl.multiple_of(index * strip, strip)
            floats = source[pl.ds(start, strip), :].astype(jnp.float32)
            inverse = lax.rsqrt(jnp.mean(floats * floats, axis=1, keepdims=True) + epsilon)
            ready[pl.ds(base + start, strip), :] = (floats * inverse * gain[...]).astype(
                jnp.bfloat16
            )
            return carry

        lax.fori_loop(0, slots // strip, norm_strip, 0)

    def column_of(share, owner):
        return jnp.sum(
            jnp.where(diagonal, jnp.broadcast_to(share[pl.ds(owner, 1), :], (slots, slots)), 0.0),
            axis=1, keepdims=True,
        )

    def widen(base, shares_in, owner, gate_block, up_block, column):
        scale = jnp.concatenate([column_of(share, owner) for share in shares_in], axis=0)
        size = slots * len(shares_in)
        values = ready[base : base + size, :]
        gate = jnp.dot(values, gate_block[...], preferred_element_type=jnp.float32)
        up = jnp.dot(values, up_block[...], preferred_element_type=jnp.float32)
        hidden[base : base + size, pl.ds(pl.multiple_of(column * width, width), width)] = (
            gate / (1.0 + jnp.exp(-gate)) * up * scale
        ).astype(jnp.bfloat16)

    def widen_group(base, shares_in, owner, side):
        block = owner * halves + side
        widen(base, shares_in, owner, gate_all.at[block], up_all.at[block], block)

    def narrow(base, size, blocks, column):
        window = slice(column * tile, (column + 1) * tile)
        total = jnp.zeros((size, tile), jnp.float32)
        for index, block in enumerate(blocks):
            total += jnp.dot(
                hidden[base : base + size, index * width : (index + 1) * width],
                block[:, window], preferred_element_type=jnp.float32,
            )
        return window, total

    group_down = [down_all.at[block] for block in range(members * halves)]

    def narrow_group(base, targets):
        for column in range(len(tiles)):
            window, total = narrow(base, slots * len(targets), group_down, column)
            for j, (target, copies) in enumerate(targets):
                target[:, window] = total[j * slots : (j + 1) * slots].astype(jnp.bfloat16)
                if copies and column < len(copies):
                    copies[column].start()

    def whole(ks, base=0):
        for owner in range(members):
            for side in range(halves):
                widen_group(base, [scales_in.at[k] for k in ks], owner, side)
        targets = []
        for k in ks:
            ready_tiles = back_copies[k] if k > 1 else None
            targets.append(((answers if k else returned).at[k], ready_tiles))
        narrow_group(base, targets)
        if 1 in ks:
            back_copies[1][0].start()

    def split(sources_in, gates, ups, downs, store):
        for i, (source, _) in enumerate(sources_in):
            norm(source, i * slots)
        shares_in = [share for _, share in sources_in]
        for side in range(halves):
            widen(0, shares_in, member, gates.at[side], ups.at[side], side)
        blocks = [downs.at[side] for side in range(halves)]
        for column in range(len(tiles)):
            window, total = narrow(0, slots * len(sources_in), blocks, column)
            store(column, window, total)

    def paired(j):
        def store(column, window, total):
            parts_out[j, :, window] = total[:slots].astype(jnp.bfloat16)
            if j == 2:
                half_copies[j][column].start()
            partial[j - 1, :, window] = total[slots:]

        return store

    def joined(j, column, target):
        window = tiles[column]
        target[:, window] = (
            partial[j - 1, :, window] + parts_in[j, :, window].astype(jnp.float32)
        ).astype(jnp.bfloat16)

    def unpack(k, window):
        return lax.dot_general(
            place[k * slots : (k + 1) * slots, :], returned[k, :, window],
            (((0,), (0,)), ((), ())), preferred_element_type=jnp.float32,
        )

    def add(k, fresh=False):
        for window in tiles:
            value = unpack(k, window)
            summed[:, window] = value if fresh else summed[:, window] + value

    def back(k):
        land(back_copies[k])
        add(k)

    def finish(k):
        for t, window in enumerate(tiles):
            back_copies[k][t].wait_recv()
            out[:, window] = (summed[:, window] + unpack(k, window)).astype(jnp.bfloat16)

    def flows(buffer, begin, count, sem):
        held = buffer.at[begin : begin + count]
        return remote(held, held, sem, back_r.at[0], twin)

    def marks(count, sem):
        held = scales.at[0:count, :members]
        return remote(held, held, sem, back_r.at[0], twin)

    @on_outer
    def _():
        for i in range(count):
            peer_copies[i].wait_recv()
            part_copies[i].start()
            near_copies[i].start()
            if i:
                part_copies[i - 1].wait_recv()
                far_copies[i - 1].start()
            if i == LATE:
                send(3)
        arrive(1)
        norm(taken.at[1], 0)
        norm(taken.at[0], slots)
        arrive(3)
        norm(taken.at[3], 2 * slots)
        part_copies[-1].wait_recv()
        far_copies[-1].start()
        for copy in group_copies:
            copy.wait()
        land(block_waits(2))
        whole((3,), 2 * slots)
        whole((1, 0))
        add(0, True)
        arrive(2)
        norm(taken.at[2], 0)
        whole((2,))
        back(1)
        half_copies[0][0].wait_recv()
        for window in tiles:
            summed[:, window] = summed[:, window] + lax.dot_general(
                place[slots : 2 * slots, :], parts_in[0, :, window],
                (((0,), (0,)), ((), ())), preferred_element_type=jnp.float32,
            )
        for t, window in enumerate(tiles):
            land([back_copies[3][t], back_copies[2][t]])
            pair = returned[2:4, :, window].reshape(2 * slots, tile)
            total = summed[:, window] + lax.dot_general(
                place[2 * slots : 4 * slots, :], pair,
                (((0,), (0,)), ((), ())), preferred_element_type=jnp.float32,
            )
            out[:, window] = total.astype(jnp.bfloat16)
        leave([flows(sent, 0, 4, row_s), marks(4, scale_s), flows(answers, 1, 3, back_s)])

    @on_inner
    def _():
        def take(begin, end):
            for i in range(begin, end):
                guest_copies[i].wait_recv()
                cross_copies[i].start()
                gnear_copies[i].start()
                if i:
                    cross_copies[i - 1].wait_recv()
                    gfar_copies[i - 1].start()

        own = own_stores

        def store_near(column, window, total):
            answers[1, :, window] = total.astype(jnp.bfloat16)

        def store_slant(column, window, total):
            parts_out[0, :, window] = total.astype(jnp.bfloat16)

        take(0, 3)
        for copy in own_copies:
            copy.wait()
        land(own_twins)
        arrive(1)
        split([(taken.at[1], scales_in.at[1])], *own, store_near)
        back_copies[1][0].start()
        take(3, 4)
        land([note_copies[1], swap_copies[1]])
        split([(extra.at[1], extra_scales.at[1]), (taken.at[0], scales_in.at[0])], *own, paired(1))
        swap(3)
        half_copies[1][0].start()
        take(4, 7)
        land([slant_scales, slant_rows])
        split([(extra.at[0], extra_scales.at[0])], *own, store_slant)
        half_copies[0][0].start()
        take(7, 10)
        arrive(2)
        swap(2)
        half_copies[1][1].start()
        take(10, count)
        cross_copies[-1].wait_recv()
        gfar_copies[-1].start()
        land(block_waits(1))
        far = [store.at[pl.ds(member * halves, halves)] for store in stores]
        land([note_copies[2], swap_copies[2]])
        split([(extra.at[2], extra_scales.at[2]), (taken.at[2], scales_in.at[2])], *far, paired(2))
        land([note_copies[3], swap_copies[3]])
        split([(extra.at[3], extra_scales.at[3]), (sent.at[3], scales.at[3])], *far, paired(3))
        half_copies[3][0].start()
        for column in range(len(tiles)):
            half_copies[2][column].wait_recv()
            joined(2, column, answers.at[2])
            back_copies[2][column].start()
        land(half_copies[1])
        for column in range(len(tiles)):
            joined(1, column, returned.at[0])
        add(0, True)
        back(1)
        land(half_copies[3])
        for column in range(len(tiles)):
            joined(3, column, returned.at[3])
        add(3)
        finish(2)
        leave([flows(sent, 0, 2, row_s), marks(2, scale_s), flows(answers, 1, 2, back_s)])
        leave([flows(sent, 0, 3, swap_s), marks(3, note_s), flows(parts_out, 0, 4, half_s)])

    leave(block_waits(3))


def group_layer(members, tokens, norm_gain, route_ids, route_weights, w_gate, w_up, w_down):
    rows, features = tokens.shape
    parts, halves = lax.axis_size("grp"), lax.axis_size("tp")
    width = w_gate.shape[2]
    slots = rows // route_ids.shape[1]
    copies = 3 * SPLIT
    blocks = members * halves
    bf16, f32, dma = jnp.bfloat16, jnp.float32, pltpu.SemaphoreType.DMA

    def vmem(*shape, dtype=bf16):
        return pltpu.VMEM(shape, dtype)

    return pl.pallas_call(
        functools.partial(group_kernel, members, parts, halves),
        out_shape=vmem(rows, features),
        in_specs=[pl.BlockSpec(memory_space=pltpu.HBM)] * 7,
        out_specs=pl.BlockSpec(memory_space=pltpu.VMEM),
        scratch_shapes=[
            vmem(1, features, dtype=f32),
            vmem(*route_ids.shape[::-1], dtype=jnp.int32),
            vmem(*route_ids.shape[::-1], dtype=f32),
            vmem(rows, features),
            vmem(GROUPS * slots, features),
            vmem(rows, features, dtype=f32),
            vmem(GROUPS * slots, rows),
            vmem(GROUPS, slots, features),
            vmem(GROUPS, slots, features),
            vmem(GROUPS, 8, slots, dtype=f32),
            vmem(GROUPS, 8, slots, dtype=f32),
            vmem(GROUPS, slots, features),
            vmem(GROUPS, slots, features),
            vmem(blocks, features, width),
            vmem(blocks, features, width),
            vmem(blocks, width, features),
            vmem(GROUPS * slots, blocks * width),
            vmem(halves, features, width),
            vmem(halves, features, width),
            vmem(halves, width, features),
            vmem(GROUPS, slots, features),
            vmem(GROUPS, 8, slots, dtype=f32),
            vmem(3, slots, features, dtype=f32),
            vmem(GROUPS, slots, features),
            vmem(GROUPS, slots, features),
            dma, dma((3,)), dma((copies,)), dma((copies,)), dma((3,)), dma((3,)), dma((3,)),
            dma, dma, dma, dma, dma, dma, dma((3,)), dma((4,)), dma((3,)), dma((4,)),
            dma((9,)), dma((8,)),
        ],
        compiler_params=pltpu.CompilerParams(
            collective_id=0, has_side_effects=True, vmem_limit_bytes=64400 * 1024
        ),
    )(
        tokens, norm_gain.reshape(1, features), route_ids.T, route_weights.T,
        w_gate[0], w_up[0], w_down[0],
    )


def solution(mesh):
    sizes = mesh.shape

    def per_device(tokens, norm_gain, route_ids, route_weights, w_gate, w_up, w_down):
        arguments = (tokens, norm_gain, route_ids, route_weights, w_gate, w_up, w_down)
        members = sizes["ep"] * w_gate.shape[0] // GROUPS
        paired = members == route_ids.shape[1] == sizes["grp"] == sizes["tp"] == 2
        if paired and w_gate.shape[0] == 1:
            return group_layer(members, *arguments)
        return general_layer(*arguments)

    in_specs = (
        P(("grp", "ep", "tp"), None),
        P(),
        P(("grp", "ep", "tp"), None),
        P(("grp", "ep", "tp"), None),
        P("ep", None, "tp"),
        P("ep", None, "tp"),
        P("ep", "tp", None),
    )
    out_specs = P(("grp", "ep", "tp"), None)
    return jax.shard_map(
        per_device, mesh=mesh, in_specs=in_specs, out_specs=out_specs, check_vma=False
    )
```
